32 devices in a mesh: sp: 16 (over z, y, core), tp: 2 (over x).
Axes of the slice: x: 2, y: 2, z: 4, core: 2. Of those that a mesh axis runs over, the one named last changes fastest.
Arguments:
- queries: bfloat16 [8192, 1024], P('sp', 'tp'), may hold values from -40 to 40
- keys_values: bfloat16 [8192, 4, 128], P('sp', 'tp'), may hold values from -40 to 40
- doc_ids: int32 [8192], P('sp'), may hold values from 0 to 3, never falling along the last dimension, each value on 1 to 4096 neighbouring positions
- head_sink: float32 [16], P('tp'), may hold values from 3 to 7
- out_weight: bfloat16 [1024, 2048], replicated, may hold values from -0.1875 to 0.1875
- hidden_in: bfloat16 [8192, 2048], P(('sp', 'tp')), may hold values from -0.59765625 to 0.59765625
- norm_gain: float32 [2048], replicated, may hold values from 0.1 to 1.9
- expert_gate: bfloat16 [32, 2048, 1024], P(('sp', 'tp')), may hold values from -0.125 to 0.125
- expert_up: bfloat16 [32, 2048, 1024], P(('sp', 'tp')), may hold values from -0.125 to 0.125
- expert_down: bfloat16 [32, 1024, 2048], P(('sp', 'tp')), may hold values from -0.1875 to 0.1875
- routes: int32 [8192, 2], P(('sp', 'tp')), may hold values from 0 to 31, all different within a row; in each aligned block of 256 rows (0 to 255, 256 to 511, ...) at most 32 rows name the same one
- route_weight: float32 [8192, 2], P(('sp', 'tp')), may hold values from 0.1 to 1
Outputs:
- layer_out: bfloat16 [8192, 2048], P(('sp', 'tp'))
The draws below stay inside these ranges and needn't reach their ends.
Inputs may be any that keep to these rules, and one draw needn't show every extreme that they name: `routes`: in the rows of one device (aligned blocks of 256 tokens in order) no expert is named more than 32 times; some expert is named exactly 32 times in some blocks.
All inputs are finite; a program needn't handle non-finite values.
Results may differ from the reference program's by a relative error of at most 0.02.
Values may be sent and summed in bfloat16 or wider, within the bound.
A program may use at most 64 MiB of HBM per device.

```python
import math
import jax
import jax.numpy as jnp
import numpy as np
from jax import lax

D = 2048
HQ = 16
KVH = 4
HD = 64
FF = 1024
TOPK = 2
WIN = 128
TOK_DEV = 512
TOKENS = 8192
EXPERTS = 32
CAP = 32
DOCS = 4
N_TP = 2


def drawn_pair(key):
    base = jax.random.fold_in(key, 11)
    query_key, pair_key = jax.random.split(base, 2)
    queries = jnp.clip(jax.random.normal(query_key, (TOKENS, HQ * HD), jnp.float32), -6.0, 6.0)
    pairs = jnp.clip(jax.random.normal(pair_key, (TOKENS, KVH, 2 * HD), jnp.float32), -6.0, 6.0)
    return (queries, pairs)


def draw_queries(key, part):
    return drawn_pair(key)[0].astype(jnp.bfloat16)


def draw_keys_values(key, part):
    return drawn_pair(key)[1].astype(jnp.bfloat16)


def level_of(own_key, shape, shards, smallest, largest):
    factor_of = 1.0
    for dim, shards_of in shards:
        steps = jax.random.uniform(jax.random.fold_in(jax.random.fold_in(own_key, 6), dim), (shards_of,), jnp.float32, smallest / len(shards), largest / len(shards))
        factor_of = factor_of * jnp.repeat(jnp.exp(steps), shape[dim] // shards_of).reshape((-1,) + (1,) * (len(shape) - 1 - dim))
    return factor_of


def length_profile(number_of, total, most, slope):
    weights = [(1 << 20) // math.isqrt(rank ** slope) + 1 for rank in range(2, number_of + 1)]
    spare, given = total - most - (number_of - 1), [1] * (number_of - 1)
    while spare > 0:
        candidates = [i for i in range(number_of - 1) if given[i] < most]
        mass, left = sum([weights[i] for i in candidates]), spare
        for i in candidates:
            extra = min(most - given[i], max(1, left * weights[i] // mass), spare)
            given[i] = given[i] + extra
            spare = spare - extra
    return np.array([most] + given)


def ragged_sizes(stream_key, amount, total, most, skew):
    if amount == 2:
        one = jax.random.randint(stream_key, (), max(1, total - most), min(most, total - 1) + 1)
        return jnp.stack([one, total - one])
    tallies = jnp.asarray(length_profile(amount, total, most, skew), jnp.int32)
    pairs = (amount - 1) // 2
    donor, taker = tallies[1:1 + 2 * pairs:2], tallies[2:2 + 2 * pairs:2]
    room = jnp.minimum(donor - 1, most - taker)
    moved = jax.random.randint(jax.random.fold_in(stream_key, 1), (pairs,), 0, 1 << 20) % (room + 1)
    tallies = tallies.at[1:1 + 2 * pairs:2].set(donor - moved).at[2:2 + 2 * pairs:2].set(taker + moved)
    return tallies[jax.random.permutation(jax.random.fold_in(stream_key, 2), amount)]


def assign_block(key, own, number, rows, amount, top, limit, lean):
    sequence = jax.random.permutation(key, amount)
    heavy_load, common = load_shares(amount, rows * top, limit, lean, True), load_shares(amount, rows * top, limit, lean, False)
    places = jnp.arange(amount)

    def named(sizes, rotation):
        used = int((sizes > 0).sum())
        fixed = max(1, used // 4)
        passed = fixed + (places - fixed + rotation * (used - fixed)) % max(1, amount - fixed)
        return jnp.zeros((amount,), jnp.int32).at[sequence[jnp.where(places < fixed, places, passed)]].set(jnp.asarray(sizes, jnp.int32))

    sizes = jnp.where(number % 4 == 0, named(heavy_load, number // 4), named(common, number - number // 4 - 1))
    mixed = jax.random.permutation(jax.random.fold_in(own, 3), amount)
    source_of, receiver = mixed[0:amount // 2 * 2:2], mixed[1:amount // 2 * 2:2]
    slack = jnp.minimum(sizes[source_of] - 1, limit - sizes[receiver]) // 2
    slack = jnp.where((source_of == sequence[0]) | (receiver == sequence[0]) | (sizes[receiver] == 0), 0, jnp.maximum(slack, 0))
    passed = jax.random.randint(jax.random.fold_in(own, 4), (amount // 2,), 0, 1 << 20) % (slack + 1)
    sizes = sizes.at[source_of].add(-passed).at[receiver].add(passed)
    members = jnp.searchsorted(jnp.cumsum(sizes), jnp.arange(rows * top), side="right").astype(jnp.int32)
    grid = members.reshape(top, rows).T
    grid = grid[jax.random.permutation(jax.random.fold_in(own, 1), rows)]
    rotation = jax.random.randint(jax.random.fold_in(own, 2), (rows, 1), 0, top)
    return jnp.take_along_axis(grid, (jnp.arange(top)[None, :] + rotation) % top, axis=1)


def load_shares(amount, total, bound, lean, full):
    portions = [(1 << 20) // math.isqrt(standing ** lean) + 1 for standing in range(1, amount + 1)]
    largest = bound if full else min(bound, max(-(-total // amount), total * portions[0] // sum(portions)))
    least = 1 if total - largest >= amount - 1 else 0
    counts, surplus = [largest] + [least] * (amount - 1), total - largest - least * (amount - 1)
    while surplus > 0:
        candidates = [i for i in range(1, amount) if counts[i] < largest] or [i for i in range(1, amount) if counts[i] < bound]
        whole, remaining = sum([portions[i] for i in candidates]), surplus
        for i in candidates:
            extra = min(bound - counts[i], max(1, remaining * portions[i] // whole), surplus)
            counts[i] = counts[i] + extra
            surplus = surplus - extra
    return np.array(counts)


def normal_values(stream_key, shape, spread, reach, cuts=(), held_as=jnp.bfloat16):
    drawn = jax.random.normal(stream_key, shape, jnp.float32) * spread
    if len(cuts) > 0:
        drawn = level_of(stream_key, shape, cuts, -0.22, 0.18) * drawn
    return jnp.clip(drawn, min=-reach, max=reach).astype(held_as)


def setup_inputs(seed: int = 0) -> dict:
    seeds = jax.random.split(jax.random.key(seed), 13)
    queries = draw_queries(jax.random.fold_in(seeds[12], 71), 0)
    keys_values = draw_keys_values(jax.random.fold_in(seeds[12], 71), 0)
    doc_ids = jnp.searchsorted(jnp.cumsum(ragged_sizes(seeds[2], DOCS, TOKENS, 8 * TOK_DEV, 1)), jnp.arange(TOKENS), side="right").astype(jnp.int32)
    head_sink = jnp.clip(3.0 + 4.0 * jax.random.uniform(seeds[3], (HQ,), jnp.float32) ** level_of(seeds[3], (HQ,), ((0, 2),), -0.2, 0.2), 3.0, 7.0)
    out_weight = normal_values(seeds[4], (HQ * HD, D), (HQ * HD) ** -0.5, 0.1875)
    hidden_in = normal_values(seeds[5], (TOKENS, D), 0.1, 0.59765625, ((0, 32),))
    norm_gain = jnp.clip(1.0 + 0.18 * jax.random.normal(seeds[6], (D,), jnp.float32), 0.1, 1.9)
    expert_gate = normal_values(seeds[7], (EXPERTS, D, FF), D ** -0.5, 0.125, ((0, 32),))
    expert_up = normal_values(seeds[8], (EXPERTS, D, FF), D ** -0.5, 0.125, ((0, 32),))
    expert_down = normal_values(seeds[9], (EXPERTS, FF, D), FF ** -0.5, 0.1875, ((0, 32),))
    routes_keys = jax.random.split(jax.random.fold_in(seeds[10], 1), TOKENS // (TOK_DEV // N_TP))
    routes_turns = jax.random.permutation(jax.random.fold_in(seeds[10], 3), TOKENS // (TOK_DEV // N_TP))
    routes = jax.vmap(lambda own, number: assign_block(jax.random.fold_in(seeds[10], 2), own, number, TOK_DEV // N_TP, EXPERTS, TOPK, CAP, 1))(routes_keys, routes_turns).reshape((TOKENS, TOPK))
    route_weight = jnp.clip(jnp.exp(math.log(1.0) - 2.3025851 * jax.random.uniform(seeds[11], (TOKENS, TOPK), jnp.float32) ** level_of(seeds[11], (TOKENS, TOPK), ((0, 32),), -0.2, 0.2)), 0.1, 1.0)
    return {"queries": queries, "keys_values": keys_values, "doc_ids": doc_ids, "head_sink": head_sink, "out_weight": out_weight, "hidden_in": hidden_in, "norm_gain": norm_gain, "expert_gate": expert_gate, "expert_up": expert_up, "expert_down": expert_down, "routes": routes, "route_weight": route_weight}


def attend_all(queries, keys_values, doc_ids, head_sink):
    span_rows = math.gcd(512, TOKENS)
    span_count = TOKENS // span_rows
    group = HQ // KVH
    padded = jnp.pad(keys_values, ((WIN, WIN), (0, 0), (0, 0)))
    padded_docs = jnp.pad(doc_ids, (WIN, WIN), constant_values=-1)
    sink_logit = head_sink.astype(jnp.float32).reshape(KVH, group)[:, :, None, None]

    def one_span(span_index):
        first_row = (span_index * span_rows).astype(jnp.int32)
        q_span = lax.dynamic_slice_in_dim(queries, first_row, span_rows, 0).astype(jnp.float32)
        q_span = q_span.reshape(span_rows, KVH, group, HD)
        kv_span = lax.dynamic_slice_in_dim(padded, first_row, span_rows + 2 * WIN, 0).astype(jnp.float32)
        key_docs = lax.dynamic_slice_in_dim(padded_docs, first_row, span_rows + 2 * WIN, 0)
        query_docs = lax.dynamic_slice_in_dim(doc_ids, first_row, span_rows, 0)
        scores = jnp.einsum('qhgd,khd->hgqk', q_span, kv_span[..., :HD]) * HD ** (-0.5)
        query_pos = first_row + jnp.arange(span_rows, dtype=jnp.int32)
        key_pos = first_row - WIN + jnp.arange(span_rows + 2 * WIN, dtype=jnp.int32)
        allowed = (jnp.abs(key_pos[None, :] - query_pos[:, None]) <= WIN) & (key_docs[None, :] == query_docs[:, None])
        masked = jnp.where(allowed, scores, -1e+30)
        row_max = jnp.maximum(masked.max(-1, keepdims=True), sink_logit)
        exp_scores = jnp.where(allowed, jnp.exp(masked - row_max), 0.0)
        total_mass = exp_scores.sum(-1, keepdims=True) + jnp.exp(sink_logit - row_max)
        weights = (exp_scores / total_mass).astype(jnp.bfloat16).astype(jnp.float32)
        outcome = jnp.einsum('hgqk,khd->qhgd', weights, kv_span[..., HD:])
        return outcome.astype(jnp.bfloat16).reshape(span_rows, HQ * HD)
    attended = lax.map(one_span, jnp.arange(span_count, dtype=jnp.int32))
    return attended.reshape(TOKENS, HQ * HD)

def expert_apply(rows_in, gate_w, up_w, down_w):
    gate = jnp.dot(rows_in, gate_w, preferred_element_type=jnp.float32)
    upper = jnp.dot(rows_in, up_w, preferred_element_type=jnp.float32)
    expert_hidden = (jax.nn.silu(gate) * upper).astype(jnp.bfloat16)
    return jnp.dot(expert_hidden, down_w, preferred_element_type=jnp.float32).astype(jnp.bfloat16)

def reference(queries, keys_values, doc_ids, head_sink, out_weight, hidden_in, norm_gain, expert_gate, expert_up, expert_down, routes, route_weight):
    attended = attend_all(queries, keys_values, doc_ids, head_sink)
    projected = jnp.dot(attended, out_weight, preferred_element_type=jnp.float32)
    mid = (hidden_in.astype(jnp.float32) + projected).astype(jnp.bfloat16)
    mid_wide = mid.astype(jnp.float32)
    normed = (mid_wide * lax.rsqrt(lax.optimization_barrier(jnp.mean(mid_wide * mid_wide, axis=-1, keepdims=True)) + 1e-06) * norm_gain.astype(jnp.float32)).astype(jnp.bfloat16)
    local_rows = TOK_DEV // N_TP
    flat_routes = routes.reshape(EXPERTS, local_rows * TOPK)
    one_hot = (flat_routes[..., None] == jnp.arange(EXPERTS, dtype=jnp.int32)).astype(jnp.int32)
    slot_rank = (jnp.cumsum(one_hot, axis=1) * one_hot).sum(-1) - 1
    owner_block = jnp.arange(EXPERTS, dtype=jnp.int32)[:, None]
    slot_index = (flat_routes * (EXPERTS * CAP) + owner_block * CAP + slot_rank).reshape(-1).astype(jnp.int32)
    repeated = jnp.repeat(normed, TOPK, axis=0)
    buffer_rows = jnp.zeros((EXPERTS * EXPERTS * CAP, D), jnp.bfloat16).at[slot_index].set(repeated)

    def per_expert(pieces):
        return expert_apply(pieces[0], pieces[1], pieces[2], pieces[3])
    results = lax.map(per_expert, (buffer_rows.reshape(EXPERTS, EXPERTS * CAP, D), expert_gate, expert_up, expert_down))
    picked = results.reshape(-1, D)[slot_index].astype(jnp.float32).reshape(TOKENS, TOPK, D)
    mixture = lax.optimization_barrier(jnp.sum(picked * route_weight.astype(jnp.float32)[..., None], axis=1))
    return (mid_wide + mixture).astype(jnp.bfloat16)
```

```python
import functools

import jax
import jax.numpy as jnp
from jax import lax
from jax.experimental import pallas as pl
from jax.experimental.pallas import tpu as pltpu
from jax.sharding import PartitionSpec as P

HD = 64
WIN = 128
PLANES = 4
CUTS = 4
TILE = 256
MESH = pl.DeviceIdType.MESH


def with_halo(cells, axis, width):
    count = lax.axis_size(axis)
    ends = count - 1
    return jnp.concatenate(
        [
            lax.ppermute(cells[-width:], axis, [(i, (i + 1) % count) for i in range(ends)]),
            cells,
            lax.ppermute(cells[:width], axis, [((i + 1) % count, i) for i in range(ends)]),
        ],
        axis=0,
    )


def place(stride, tps):
    sp = lax.axis_index("sp")
    tp = lax.axis_index("tp")
    return lax.div(sp, stride), lax.rem(sp, stride), tp, lax.rem(sp, stride) * tps + tp


def greet(z, r, tp, p, planes, stride, tps):
    peers = stride * tps
    barrier = pltpu.get_barrier_semaphore()
    for k in range(1, peers):
        pd = lax.rem(p + k, peers)
        pl.semaphore_signal(
            barrier,
            inc=1,
            device_id=(z * stride + lax.div(pd, tps), lax.rem(pd, tps)),
            device_id_type=MESH,
        )

    @pl.when(z > 0)
    def _():
        pl.semaphore_signal(
            barrier, inc=1, device_id=((z - 1) * stride + r, tp), device_id_type=MESH
        )

    @pl.when(z < planes - 1)
    def _():
        pl.semaphore_signal(
            barrier, inc=1, device_id=((z + 1) * stride + r, tp), device_id_type=MESH
        )

    beside = (z > 0).astype(jnp.int32) + (z < planes - 1).astype(jnp.int32)
    pl.semaphore_wait(barrier, peers - 1 + beside)


def slot_hits(tab, z, slots, rows):
    ids = lax.broadcasted_iota(jnp.int32, (slots, rows), 0) + z * slots
    ids = ids.astype(jnp.float32)
    return ids == tab[0:1, :], ids == tab[1:2, :]


def layer_kernel(
    planes, stride, tps, cap,
    x_ref, tab_ref, mid_ref, gate_ref, up_ref, down_ref, out_ref,
    toks, stage, land, results, held, part, from_low, from_high,
    gate_w, up_w, down_w, hidden, mixer, total, tabs,
    zsend, zrecv, psend, precv, rsend, rrecv, csend, lowrecv, highrecv, tsend, trecv, wsem,
):
    z, r, tp, p = place(stride, tps)
    peers = stride * tps
    rows, width = x_ref.shape
    cols = width // CUTS
    slots = peers * cap
    near = planes - 1
    greet(z, r, tp, p, planes, stride, tps)

    def span(h):
        return pl.ds(pl.multiple_of(h * cols, cols), cols)

    def seat(k):
        return pl.ds(pl.multiple_of(k * cap, cap), cap)

    def beside(side):
        return ((z + 1 - 2 * side) * stride + r, tp)

    def fellow(k):
        return (z * stride + lax.div(k, tps), lax.rem(k, tps))

    def hop(zs, h, side):
        return pltpu.make_async_remote_copy(
            src_ref=toks.at[zs, :, span(h)],
            dst_ref=toks.at[zs, :, span(h)],
            send_sem=zsend.at[side, zs, h],
            recv_sem=zrecv.at[zs, h],
            device_id=beside(side),
            device_id_type=MESH,
        )

    def own_hop(h, side):
        return pltpu.make_async_remote_copy(
            src_ref=x_ref.at[:, span(h)],
            dst_ref=toks.at[z, :, span(h)],
            send_sem=zsend.at[side, z, h],
            recv_sem=zrecv.at[z, h],
            device_id=beside(side),
            device_id_type=MESH,
        )

    def tab_hop(zs, side, source):
        return pltpu.make_async_remote_copy(
            src_ref=source,
            dst_ref=tabs.at[zs],
            send_sem=tsend.at[side, zs],
            recv_sem=trecv.at[zs],
            device_id=beside(side),
            device_id_type=MESH,
        )

    def give(zs, h, dest, at):
        return pltpu.make_async_remote_copy(
            src_ref=stage.at[zs, seat(dest), span(h)],
            dst_ref=land.at[zs, seat(at), span(h)],
            send_sem=psend.at[zs, h, dest],
            recv_sem=precv.at[zs, h, at],
            device_id=fellow(dest),
            device_id_type=MESH,
        )

    def back(zs, h, dest, at):
        return pltpu.make_async_remote_copy(
            src_ref=results.at[zs, seat(dest), span(h)],
            dst_ref=held.at[zs, seat(at), span(h)],
            send_sem=rsend.at[zs, h, dest],
            recv_sem=rrecv.at[zs, h, at],
            device_id=fellow(dest),
            device_id_type=MESH,
        )

    def climb(zs, h):
        return pltpu.make_async_remote_copy(
            src_ref=part.at[zs, :, span(h)],
            dst_ref=from_low.at[zs, :, span(h)],
            send_sem=csend.at[zs, h],
            recv_sem=lowrecv.at[zs, h],
            device_id=beside(0),
            device_id_type=MESH,
        )

    def sink(zs, h):
        return pltpu.make_async_remote_copy(
            src_ref=part.at[zs, :, span(h)],
            dst_ref=from_high.at[zs, :, span(h)],
            send_sem=csend.at[zs, h],
            recv_sem=highrecv.at[zs, h],
            device_id=beside(1),
            device_id_type=MESH,
        )

    loads = [
        pltpu.make_async_copy(source, target, wsem.at[k])
        for k, (source, target) in enumerate(
            [(gate_ref, gate_w), (up_ref, up_w), (down_ref, down_w)]
        )
    ]

    def pack(block, zs, h):
        first, second = slot_hits(tabs[zs], z, slots, rows)
        pick = jnp.where(first | second, 1.0, 0.0).astype(jnp.bfloat16)
        picked = jnp.dot(pick, block, preferred_element_type=jnp.float32)
        stage[zs, :, span(h)] = picked.astype(jnp.bfloat16)
        for k in range(1, peers):
            give(zs, h, lax.rem(p + k, peers), p).start()
        land[zs, seat(p), span(h)] = stage[zs, seat(p), span(h)]

    def experts(zs):
        tab = tabs[zs]
        first, second = slot_hits(tab, z, slots, rows)
        mix = jnp.where(first, tab[2:3, :], 0.0) + jnp.where(second, tab[3:4, :], 0.0)
        mixer[zs] = mix.T.astype(jnp.bfloat16)

        @pl.loop(0, CUTS)
        def _(h):
            for k in range(1, peers):
                other = lax.rem(p + k, peers)
                give(zs, h, other, other).wait_recv()

        @pl.loop(0, gate_w.shape[1] // TILE)
        def _(c):
            at = pl.ds(pl.multiple_of(c * TILE, TILE), TILE)
            gate = jnp.dot(land[zs], gate_w[:, at], preferred_element_type=jnp.float32)
            upper = jnp.dot(land[zs], up_w[:, at], preferred_element_type=jnp.float32)
            hidden[:, at] = (gate / (1.0 + jnp.exp(-gate)) * upper).astype(jnp.bfloat16)

        @pl.loop(0, CUTS)
        def _(h):
            @pl.loop(0, cols // TILE)
            def _(c):
                at = pl.ds(pl.multiple_of(h * cols + c * TILE, TILE), TILE)
                results[zs, :, at] = jnp.dot(
                    hidden[...], down_w[:, at], preferred_element_type=jnp.float32
                ).astype(jnp.bfloat16)

            for k in range(1, peers):
                back(zs, h, lax.rem(p + k, peers), p).start()
            held[zs, seat(p), span(h)] = results[zs, seat(p), span(h)]

    def mixed(zs, h):
        for k in range(1, peers):
            back(zs, h, p, lax.rem(p + k, peers)).wait_recv()
        return jnp.dot(mixer[zs], held[zs, :, span(h)], preferred_element_type=jnp.float32)

    def homeward(stage_of, h):
        @pl.loop(0, 2)
        def _(k):
            down = (k == 0) == (z >= planes // 2)
            zs = jnp.where(down, near - stage_of, stage_of)

            @pl.when(down & (zs < z))
            def _():
                part[zs, :, span(h)] = mixed(zs, h).astype(jnp.bfloat16)

                @pl.when(z < near)
                def _():
                    sink(zs, h).wait_recv()
                    part[zs, :, span(h)] += from_high[zs, :, span(h)]

                sink(zs, h).start()

            @pl.when(jnp.logical_not(down) & (zs > z))
            def _():
                part[zs, :, span(h)] = mixed(zs, h).astype(jnp.bfloat16)

                @pl.when(z > 0)
                def _():
                    climb(zs, h).wait_recv()
                    part[zs, :, span(h)] += from_low[zs, :, span(h)]

                climb(zs, h).start()

    @pl.when(z < near)
    def _():
        tab_hop(z, 0, tab_ref).start()

    @pl.when(z > 0)
    def _():
        tab_hop(z, 1, tab_ref).start()

    for h in range(CUTS):

        @pl.when(z < near)
        def _():
            own_hop(h, 0).start()

        @pl.when(z > 0)
        def _():
            own_hop(h, 1).start()

    for load in loads:
        load.start()
    tabs[z] = tab_ref[...]

    @pl.loop(0, CUTS)
    def _(h):
        pack(x_ref[:, span(h)], z, h)

    for load in loads:
        load.wait()

    @pl.loop(CUTS, (planes + 1) * CUTS)
    def _(e):
        dist = lax.div(e, CUTS)
        h = lax.rem(e, CUTS)

        @pl.loop(0, 2)
        def _(side):
            zs = z - dist + 2 * dist * side
            onward = z + 1 - 2 * side

            @pl.when((zs >= 0) & (zs < planes))
            def _():
                @pl.when(h == 0)
                def _():
                    tab_hop(zs, side, tabs.at[zs]).wait_recv()

                    @pl.when((onward >= 0) & (onward < planes))
                    def _():
                        tab_hop(zs, side, tabs.at[zs]).start()

                hop(zs, h, side).wait_recv()

                @pl.when((onward >= 0) & (onward < planes))
                def _():
                    hop(zs, h, side).start()

                pack(toks[zs, :, span(h)], zs, h)

        @pl.when(h == 0)
        def _():
            @pl.loop(0, 2)
            def _(side):
                zs = z - (dist - 1) + 2 * (dist - 1) * side

                @pl.when((zs >= 0) & (zs < planes) & ((dist > 1) | (side == 0)))
                def _():
                    experts(zs)

        @pl.when((dist > 1) & (h > 0))
        def _():
            homeward(dist - 1, h - 1)

        @pl.when((dist > 1) & (h == CUTS - 1))
        def _():
            homeward(dist - 1, h)

        @pl.when(dist == planes - 1)
        def _():
            total[:, span(h)] = mid_ref[:, span(h)].astype(jnp.float32) + mixed(z, h)

    @pl.loop(0, CUTS)
    def _(h):
        @pl.when(z > 0)
        def _():
            climb(z, h).wait_recv()
            total[:, span(h)] += from_low[z, :, span(h)].astype(jnp.float32)

        @pl.when(z < near)
        def _():
            sink(z, h).wait_recv()
            total[:, span(h)] += from_high[z, :, span(h)].astype(jnp.float32)

        out_ref[:, span(h)] = total[:, span(h)].astype(jnp.bfloat16)

    @pl.loop(0, planes * CUTS)
    def _(e):
        zs = lax.div(e, CUTS)
        h = lax.rem(e, CUTS)

        @pl.when((zs <= z) & (z < near))
        def _():
            hop(zs, h, 0).wait_send()

        @pl.when((zs >= z) & (z > 0))
        def _():
            hop(zs, h, 1).wait_send()

        @pl.when(zs > z)
        def _():
            climb(zs, h).wait_send()

        @pl.when(zs < z)
        def _():
            sink(zs, h).wait_send()

        for k in range(1, peers):
            give(zs, h, lax.rem(p + k, peers), p).wait_send()
            back(zs, h, lax.rem(p + k, peers), p).wait_send()

        @pl.when(h == 0)
        def _():
            @pl.when((zs <= z) & (z < near))
            def _():
                tab_hop(zs, 0, tabs.at[zs]).wait_send()

            @pl.when((zs >= z) & (z > 0))
            def _():
                tab_hop(zs, 1, tabs.at[zs]).wait_send()


def routed_by_plane(normed, mid, tab, planes, cap, weights):
    rows, width = normed.shape
    tps = lax.axis_size("tp")
    stride = lax.axis_size("sp") // planes
    peers = stride * tps
    slots = peers * cap
    dma = pltpu.SemaphoreType.DMA
    vmem = pl.BlockSpec(memory_space=pltpu.VMEM)
    anywhere = pl.BlockSpec(memory_space=pl.ANY)
    hidden = weights[0].shape[1]
    by_slot = pltpu.VMEM((planes, slots, width), jnp.bfloat16)
    by_row = pltpu.VMEM((planes, rows, width), jnp.bfloat16)
    chunks = dma((planes, CUTS))
    fans = dma((planes, CUTS, peers))
    return pl.pallas_call(
        functools.partial(layer_kernel, planes, stride, tps, cap),
        out_shape=jax.ShapeDtypeStruct((rows, width), jnp.bfloat16),
        in_specs=[vmem, vmem, vmem, anywhere, anywhere, anywhere],
        out_specs=vmem,
        scratch_shapes=[
            by_row, by_slot, by_slot, by_slot, by_slot, by_row, by_row, by_row,
            pltpu.VMEM((width, hidden), jnp.bfloat16),
            pltpu.VMEM((width, hidden), jnp.bfloat16),
            pltpu.VMEM((hidden, width), jnp.bfloat16),
            pltpu.VMEM((slots, hidden), jnp.bfloat16),
            pltpu.VMEM((planes, rows, slots), jnp.bfloat16),
            pltpu.VMEM((rows, width), jnp.float32),
            pltpu.VMEM((planes,) + tab.shape, jnp.float32),
            dma((2, planes, CUTS)), chunks, fans, fans, fans, fans, chunks, chunks, chunks,
            dma((2, planes)), dma((planes,)), dma((3,)),
        ],
        compiler_params=pltpu.CompilerParams(
            collective_id=0, has_side_effects=True, vmem_limit_bytes=60 * 1024 * 1024
        ),
        name="routed",
    )(normed, tab, mid, *weights)


def expert_rows(arrived, gate_w, up_w, down_w):
    width = arrived.shape[-1]
    flat_rows = arrived.reshape(-1, width)
    gate = jnp.dot(flat_rows, gate_w, preferred_element_type=jnp.float32)
    upper = jnp.dot(flat_rows, up_w, preferred_element_type=jnp.float32)
    expert_hidden = (jax.nn.silu(gate) * upper).astype(jnp.bfloat16)
    result = jnp.dot(expert_hidden, down_w, preferred_element_type=jnp.float32).astype(jnp.bfloat16)
    return result.reshape(arrived.shape[:-1] + (result.shape[-1],))


def shards(
    queries,
    keys_values,
    doc_ids,
    head_sink,
    out_weight,
    hidden_in,
    norm_gain,
    expert_gate,
    expert_up,
    expert_down,
    routes,
    route_weight,
):
    tok_here = queries.shape[0]
    heads_here = head_sink.shape[0]
    kv_here = keys_values.shape[1]
    group = heads_here // kv_here
    head_dim = keys_values.shape[2] // 2
    docs_wide = jnp.broadcast_to(
        doc_ids.astype(jnp.bfloat16)[:, None], (tok_here, keys_values.shape[2])
    )
    slab = jnp.concatenate([keys_values.reshape(tok_here, -1), docs_wide], axis=1)
    slab = with_halo(slab, "sp", WIN)
    kv_ext = slab[:, : kv_here * keys_values.shape[2]].reshape(
        -1, kv_here, keys_values.shape[2]
    )
    docs_ext = slab[:, kv_here * keys_values.shape[2]].astype(jnp.int32)
    offset = lax.axis_index("sp") * tok_here
    seq_total = lax.axis_size("sp") * tok_here
    span_rows = min(512, tok_here)
    sink_logit = head_sink.reshape(kv_here, group)[:, :, None, None]

    def one_span(span_index):
        first_row = span_index * span_rows
        q_span = queries.reshape(span_rows, kv_here, group, head_dim)
        scores = jnp.einsum(
            "qhgd,khd->hgqk", q_span, kv_ext[..., :head_dim], preferred_element_type=jnp.float32
        ) * HD ** (-0.5)
        query_pos = offset + first_row + jnp.arange(span_rows, dtype=jnp.int32)
        key_pos = offset + first_row - WIN + jnp.arange(span_rows + 2 * WIN, dtype=jnp.int32)
        inside = (key_pos >= 0) & (key_pos < seq_total)
        allowed = (
            (jnp.abs(key_pos[None, :] - query_pos[:, None]) <= WIN)
            & inside[None, :]
            & (docs_ext[None, :] == doc_ids[:, None])
        )
        masked = jnp.where(allowed, scores, -1e30)
        row_max = jnp.maximum(masked.max(-1, keepdims=True), sink_logit)
        exp_scores = jnp.where(allowed, jnp.exp(masked - row_max), 0.0)
        total_mass = exp_scores.sum(-1, keepdims=True) + jnp.exp(sink_logit - row_max)
        weights = (exp_scores / total_mass).astype(jnp.bfloat16)
        outcome = jnp.einsum(
            "hgqk,khd->qhgd", weights, kv_ext[..., head_dim:], preferred_element_type=jnp.float32
        )
        return outcome.astype(jnp.bfloat16).reshape(span_rows, heads_here * head_dim)

    attended = lax.map(one_span, jnp.arange(tok_here // span_rows, dtype=jnp.int32)).reshape(
        tok_here, -1
    )
    if lax.axis_size("tp") == 2:
        tp = lax.axis_index("tp")
        half = tok_here // 2
        mine = lax.dynamic_slice_in_dim(attended, tp * half, half, 0)
        other = lax.ppermute(
            lax.dynamic_slice_in_dim(attended, (1 - tp) * half, half, 0), "tp", [(0, 1), (1, 0)]
        )
        gathered = jnp.concatenate(
            [jnp.where(tp == 0, mine, other), jnp.where(tp == 0, other, mine)], axis=1
        )
    else:
        gathered = lax.all_to_all(attended, "tp", split_axis=0, concat_axis=1, tiled=True)
    projected = jnp.dot(gathered, out_weight, preferred_element_type=jnp.float32)
    mid_wide = (hidden_in.astype(jnp.float32) + projected).astype(jnp.bfloat16).astype(jnp.float32)
    normed = (
        mid_wide
        * lax.rsqrt(jnp.mean(mid_wide * mid_wide, axis=-1, keepdims=True) + 1e-06)
        * norm_gain
    ).astype(jnp.bfloat16)
    local_rows = normed.shape[0]
    topk = routes.shape[1]
    width = normed.shape[1]
    sp_count = lax.axis_size("sp")
    tp_count = lax.axis_size("tp")
    expert_count = sp_count * tp_count
    capacity = 2 * local_rows * topk // expert_count
    flat_routes = routes.reshape(-1)
    one_hot = (flat_routes[:, None] == jnp.arange(expert_count, dtype=jnp.int32)[None, :]).astype(
        jnp.int32
    )
    slot_rank = (jnp.cumsum(one_hot, axis=0) * one_hot).sum(-1) - 1
    slot_index = flat_routes * capacity + slot_rank
    if capacity % 16 == 0 and sp_count % PLANES == 0 and topk == 2:
        tab = jnp.concatenate(
            [
                slot_index.reshape(local_rows, topk).astype(jnp.float32).T,
                route_weight.T,
                jnp.zeros((4, local_rows), jnp.float32),
            ],
            axis=0,
        )
        return routed_by_plane(
            normed,
            mid_wide.astype(jnp.bfloat16),
            tab,
            PLANES,
            capacity,
            (expert_gate[0], expert_up[0], expert_down[0]),
        )
    repeated = jnp.repeat(normed, topk, axis=0)
    buffer_rows = (
        jnp.zeros((expert_count * capacity, width), jnp.bfloat16).at[slot_index].set(repeated)
    )
    sent = buffer_rows.reshape(expert_count, capacity, width)
    finished = expert_rows(
        lax.all_to_all(sent, ("sp", "tp"), split_axis=0, concat_axis=0, tiled=True),
        expert_gate[0],
        expert_up[0],
        expert_down[0],
    )
    returned = lax.all_to_all(finished, ("sp", "tp"), split_axis=0, concat_axis=0, tiled=True)
    returned = returned.reshape(expert_count * capacity, width)
    picked = returned[slot_index].astype(jnp.float32).reshape(local_rows, topk, width)
    mixture = jnp.sum(picked * route_weight[..., None], axis=1)
    return (mid_wide + mixture).astype(jnp.bfloat16)


def solution(mesh):
    placed = (
        P("sp", "tp"),
        P("sp", "tp", None),
        P("sp"),
        P("tp"),
        P(),
        P(("sp", "tp"), None),
        P(),
        P(("sp", "tp"), None, None),
        P(("sp", "tp"), None, None),
        P(("sp", "tp"), None, None),
        P(("sp", "tp"), None),
        P(("sp", "tp"), None),
    )
    return jax.shard_map(
        shards, mesh=mesh, in_specs=placed, out_specs=P(("sp", "tp"), None), check_vma=False
    )
```

```python
import functools

import jax
import jax.numpy as jnp
from jax import lax
from jax.experimental import pallas as pl
from jax.experimental.pallas import tpu as pltpu
from jax.sharding import PartitionSpec as P

HD = 64
WIN = 128
PLANES = 4
CUTS = 8
TILE = 256
LAND_LAG = 2
HELD_LAG = 2
FAR_LAG = 2
MESH = pl.DeviceIdType.MESH


def with_halo(cells, axis, width):
    count = lax.axis_size(axis)
    ends = count - 1
    return jnp.concatenate(
        [
            lax.ppermute(cells[-width:], axis, [(i, (i + 1) % count) for i in range(ends)]),
            cells,
            lax.ppermute(cells[:width], axis, [((i + 1) % count, i) for i in range(ends)]),
        ],
        axis=0,
    )


def place(stride, tps):
    sp = lax.axis_index("sp")
    tp = lax.axis_index("tp")
    return lax.div(sp, stride), lax.rem(sp, stride), tp, lax.rem(sp, stride) * tps + tp


def greet(z, r, tp, p, planes, stride, tps):
    peers = stride * tps
    barrier = pltpu.get_barrier_semaphore()
    for k in range(1, peers):
        pd = lax.rem(p + k, peers)
        pl.semaphore_signal(
            barrier,
            inc=1,
            device_id=(z * stride + lax.div(pd, tps), lax.rem(pd, tps)),
            device_id_type=MESH,
        )

    @pl.when(z > 0)
    def _():
        pl.semaphore_signal(
            barrier, inc=1, device_id=((z - 1) * stride + r, tp), device_id_type=MESH
        )

    @pl.when(z < planes - 1)
    def _():
        pl.semaphore_signal(
            barrier, inc=1, device_id=((z + 1) * stride + r, tp), device_id_type=MESH
        )

    beside = (z > 0).astype(jnp.int32) + (z < planes - 1).astype(jnp.int32)
    pl.semaphore_wait(barrier, peers - 1 + beside)


def slot_hits(tab, z, slots, rows):
    ids = lax.broadcasted_iota(jnp.int32, (slots, rows), 0) + z * slots
    ids = ids.astype(jnp.float32)
    return ids == tab[0:1, :], ids == tab[1:2, :]


def layer_kernel(
    planes, stride, tps, cap,
    x_ref, tab_ref, mid_ref, gate_ref, up_ref, down_ref, out_ref,
    toks, stage, land, results, held, part, from_low, from_high,
    gate_w, up_w, down_w, gate_sum, up_sum, hidden, mixer, total, tabs,
    zsend, zrecv, psend, precv, rsend, rrecv, csend, lowrecv, highrecv, tsend, trecv, wsem,
):
    z, r, tp, p = place(stride, tps)
    peers = stride * tps
    rows, width = x_ref.shape
    cols = width // CUTS
    slots = peers * cap
    near = planes - 1
    packed = planes * CUTS
    greet(z, r, tp, p, planes, stride, tps)

    def block(b):
        inward = jnp.where(z < planes // 2, z + b, z - b)
        outward = jnp.where(z < planes // 2, z - 1, z + 1)
        return jnp.where((inward >= 0) & (inward < planes), inward, outward)

    def span(h):
        return pl.ds(pl.multiple_of(h * cols, cols), cols)

    def seat(k):
        return pl.ds(pl.multiple_of(k * cap, cap), cap)

    def beside(side):
        return ((z + 1 - 2 * side) * stride + r, tp)

    def fellow(k):
        return (z * stride + lax.div(k, tps), lax.rem(k, tps))

    def hop(zs, h, side):
        return pltpu.make_async_remote_copy(
            src_ref=toks.at[zs, :, span(h)],
            dst_ref=toks.at[zs, :, span(h)],
            send_sem=zsend.at[side, zs, h],
            recv_sem=zrecv.at[zs, h],
            device_id=beside(side),
            device_id_type=MESH,
        )

    def own_hop(h, side):
        return pltpu.make_async_remote_copy(
            src_ref=x_ref.at[:, span(h)],
            dst_ref=toks.at[z, :, span(h)],
            send_sem=zsend.at[side, z, h],
            recv_sem=zrecv.at[z, h],
            device_id=beside(side),
            device_id_type=MESH,
        )

    def tab_hop(zs, side, source):
        return pltpu.make_async_remote_copy(
            src_ref=source,
            dst_ref=tabs.at[zs],
            send_sem=tsend.at[side, zs],
            recv_sem=trecv.at[zs],
            device_id=beside(side),
            device_id_type=MESH,
        )

    def give(zs, h, dest, at):
        return pltpu.make_async_remote_copy(
            src_ref=stage.at[zs, seat(dest), span(h)],
            dst_ref=land.at[zs, seat(at), span(h)],
            send_sem=psend.at[zs, h, dest],
            recv_sem=precv.at[zs, h, at],
            device_id=fellow(dest),
            device_id_type=MESH,
        )

    def back(zs, h, dest, at):
        return pltpu.make_async_remote_copy(
            src_ref=results.at[zs, seat(dest), span(h)],
            dst_ref=held.at[zs, seat(at), span(h)],
            send_sem=rsend.at[zs, h, dest],
            recv_sem=rrecv.at[zs, h, at],
            device_id=fellow(dest),
            device_id_type=MESH,
        )

    def climb(zs, h):
        return pltpu.make_async_remote_copy(
            src_ref=part.at[zs, :, span(h)],
            dst_ref=from_low.at[zs, :, span(h)],
            send_sem=csend.at[zs, h],
            recv_sem=lowrecv.at[zs, h],
            device_id=beside(0),
            device_id_type=MESH,
        )

    def sink(zs, h):
        return pltpu.make_async_remote_copy(
            src_ref=part.at[zs, :, span(h)],
            dst_ref=from_high.at[zs, :, span(h)],
            send_sem=csend.at[zs, h],
            recv_sem=highrecv.at[zs, h],
            device_id=beside(1),
            device_id_type=MESH,
        )

    loads = [
        pltpu.make_async_copy(source, target, wsem.at[k])
        for k, (source, target) in enumerate(
            [(gate_ref, gate_w), (up_ref, up_w), (down_ref, down_w)]
        )
    ]

    def pack(zs, h):
        first, second = slot_hits(tabs[zs], z, slots, rows)
        pick = jnp.where(first | second, 1.0, 0.0).astype(jnp.bfloat16)
        picked = jnp.dot(pick, toks[zs, :, span(h)], preferred_element_type=jnp.float32)
        stage[zs, :, span(h)] = picked.astype(jnp.bfloat16)
        for k in range(1, peers):
            give(zs, h, lax.rem(p + k, peers), p).start()
        land[zs, seat(p), span(h)] = stage[zs, seat(p), span(h)]

    def expand(zs, h):
        @pl.when(h == 0)
        def _():
            tab = tabs[zs]
            first, second = slot_hits(tab, z, slots, rows)
            mix = jnp.where(first, tab[2:3, :], 0.0) + jnp.where(second, tab[3:4, :], 0.0)
            mixer[zs] = mix.T.astype(jnp.bfloat16)
            gate_sum[...] = jnp.zeros_like(gate_sum)
            up_sum[...] = jnp.zeros_like(up_sum)

        for k in range(1, peers):
            other = lax.rem(p + k, peers)
            give(zs, h, other, other).wait_recv()

        @pl.loop(0, gate_w.shape[1] // TILE)
        def _(c):
            at = pl.ds(pl.multiple_of(c * TILE, TILE), TILE)
            here = land[zs, :, span(h)]
            gate_sum[:, at] += jnp.dot(
                here, gate_w[span(h), at], preferred_element_type=jnp.float32
            )
            up_sum[:, at] += jnp.dot(here, up_w[span(h), at], preferred_element_type=jnp.float32)

        @pl.when(h == CUTS - 1)
        def _():
            @pl.loop(0, gate_w.shape[1] // TILE)
            def _(c):
                at = pl.ds(pl.multiple_of(c * TILE, TILE), TILE)
                gate = gate_sum[:, at]
                hidden[:, at] = (gate / (1.0 + jnp.exp(-gate)) * up_sum[:, at]).astype(
                    jnp.bfloat16
                )

    def contract(zs, h):
        results[zs, :, span(h)] = jnp.dot(
            hidden[...], down_w[:, span(h)], preferred_element_type=jnp.float32
        ).astype(jnp.bfloat16)

    def send_back(zs, h):
        for k in range(1, peers):
            back(zs, h, lax.rem(p + k, peers), p).start()
        held[zs, seat(p), span(h)] = results[zs, seat(p), span(h)]

    def mixed(zs, h):
        for k in range(1, peers):
            back(zs, h, p, lax.rem(p + k, peers)).wait_recv()
        return jnp.dot(mixer[zs], held[zs, :, span(h)], preferred_element_type=jnp.float32)

    def homeward(f):
        @pl.loop(0, 2)
        def _(k):
            down = (k == 0) == (z >= planes // 2)
            g = f - FAR_LAG * k
            round_of = lax.div(g, CUTS) + 1
            h = lax.rem(g, CUTS)
            zs = jnp.where(down, near - round_of, round_of)
            due = (g >= 0) & (g < near * CUTS)

            @pl.when(due & down & (zs < z))
            def _():
                mine = mixed(zs, h)

                @pl.when(z == near)
                def _():
                    part[zs, :, span(h)] = mine.astype(jnp.bfloat16)

                @pl.when(z < near)
                def _():
                    sink(zs, h).wait_recv()
                    above = from_high[zs, :, span(h)].astype(jnp.float32)
                    part[zs, :, span(h)] = (mine + above).astype(jnp.bfloat16)

                sink(zs, h).start()

            @pl.when(due & jnp.logical_not(down) & (zs > z))
            def _():
                mine = mixed(zs, h)

                @pl.when(z == 0)
                def _():
                    part[zs, :, span(h)] = mine.astype(jnp.bfloat16)

                @pl.when(z > 0)
                def _():
                    climb(zs, h).wait_recv()
                    below = from_low[zs, :, span(h)].astype(jnp.float32)
                    part[zs, :, span(h)] = (mine + below).astype(jnp.bfloat16)

                climb(zs, h).start()

    @pl.when(z < near)
    def _():
        tab_hop(z, 0, tab_ref).start()

    @pl.when(z > 0)
    def _():
        tab_hop(z, 1, tab_ref).start()

    for h in range(CUTS):

        @pl.when(z < near)
        def _():
            own_hop(h, 0).start()

        @pl.when(z > 0)
        def _():
            own_hop(h, 1).start()

    for load in loads:
        load.start()
    tabs[z] = tab_ref[...]

    toks[z] = x_ref[...]

    @pl.loop(0, CUTS)
    def _(h):
        pack(z, h)

    for load in loads:
        load.wait()

    def turn(k):
        nth = lax.div(k, CUTS)
        return jnp.where(nth < near, block(nth + 1), z), lax.rem(k, CUTS)

    @pl.loop(0, packed + LAND_LAG + CUTS - 1)
    def _(e):
        dist = lax.div(e, CUTS) + 1
        h = lax.rem(e, CUTS)

        @pl.when(dist <= near)
        def _():
            @pl.loop(0, 2)
            def _(side):
                zs = z - dist + 2 * dist * side
                onward = z + 1 - 2 * side

                @pl.when((zs >= 0) & (zs < planes))
                def _():
                    @pl.when(h == 0)
                    def _():
                        tab_hop(zs, side, tabs.at[zs]).wait_recv()

                        @pl.when((onward >= 0) & (onward < planes))
                        def _():
                            tab_hop(zs, side, tabs.at[zs]).start()

                    hop(zs, h, side).wait_recv()

                    @pl.when((onward >= 0) & (onward < planes))
                    def _():
                        hop(zs, h, side).start()

            pack(block(dist), h)

        g = e - LAND_LAG

        @pl.when((g >= 0) & (g < packed))
        def _():
            expand(*turn(g))

        c = g - CUTS + 1

        @pl.when(c >= 0)
        def _():
            contract(*turn(c))
            send_back(*turn(c))

        homeward(c - HELD_LAG)

    @pl.loop(0, CUTS)
    def _(h):
        total[:, span(h)] = mid_ref[:, span(h)].astype(jnp.float32) + mixed(z, h)

        @pl.when(z > 0)
        def _():
            climb(z, h).wait_recv()
            total[:, span(h)] += from_low[z, :, span(h)].astype(jnp.float32)

        @pl.when(z < near)
        def _():
            sink(z, h).wait_recv()
            total[:, span(h)] += from_high[z, :, span(h)].astype(jnp.float32)

        out_ref[:, span(h)] = total[:, span(h)].astype(jnp.bfloat16)

    @pl.loop(0, planes * CUTS)
    def _(e):
        zs = lax.div(e, CUTS)
        h = lax.rem(e, CUTS)

        @pl.when((zs <= z) & (z < near))
        def _():
            hop(zs, h, 0).wait_send()

        @pl.when((zs >= z) & (z > 0))
        def _():
            hop(zs, h, 1).wait_send()

        @pl.when(zs > z)
        def _():
            climb(zs, h).wait_send()

        @pl.when(zs < z)
        def _():
            sink(zs, h).wait_send()

        for k in range(1, peers):
            give(zs, h, lax.rem(p + k, peers), p).wait_send()
            back(zs, h, lax.rem(p + k, peers), p).wait_send()

        @pl.when(h == 0)
        def _():
            @pl.when((zs <= z) & (z < near))
            def _():
                tab_hop(zs, 0, tabs.at[zs]).wait_send()

            @pl.when((zs >= z) & (z > 0))
            def _():
                tab_hop(zs, 1, tabs.at[zs]).wait_send()


def routed_by_plane(normed, mid, tab, planes, cap, weights):
    rows, width = normed.shape
    tps = lax.axis_size("tp")
    stride = lax.axis_size("sp") // planes
    peers = stride * tps
    slots = peers * cap
    dma = pltpu.SemaphoreType.DMA
    vmem = pl.BlockSpec(memory_space=pltpu.VMEM)
    anywhere = pl.BlockSpec(memory_space=pl.ANY)
    hidden = weights[0].shape[1]
    by_slot = pltpu.VMEM((planes, slots, width), jnp.bfloat16)
    by_row = pltpu.VMEM((planes, rows, width), jnp.bfloat16)
    chunks = dma((planes, CUTS))
    fans = dma((planes, CUTS, peers))
    return pl.pallas_call(
        functools.partial(layer_kernel, planes, stride, tps, cap),
        out_shape=jax.ShapeDtypeStruct((rows, width), jnp.bfloat16),
        in_specs=[vmem, vmem, vmem, anywhere, anywhere, anywhere],
        out_specs=vmem,
        scratch_shapes=[
            by_row, by_slot, by_slot, by_slot, by_slot, by_row, by_row, by_row,
            pltpu.VMEM((width, hidden), jnp.bfloat16),
            pltpu.VMEM((width, hidden), jnp.bfloat16),
            pltpu.VMEM((hidden, width), jnp.bfloat16),
            pltpu.VMEM((slots, hidden), jnp.float32),
            pltpu.VMEM((slots, hidden), jnp.float32),
            pltpu.VMEM((slots, hidden), jnp.bfloat16),
            pltpu.VMEM((planes, rows, slots), jnp.bfloat16),
            pltpu.VMEM((rows, width), jnp.float32),
            pltpu.VMEM((planes,) + tab.shape, jnp.float32),
            dma((2, planes, CUTS)), chunks, fans, fans, fans, fans, chunks, chunks, chunks,
            dma((2, planes)), dma((planes,)), dma((3,)),
        ],
        compiler_params=pltpu.CompilerParams(
            collective_id=0, has_side_effects=True, vmem_limit_bytes=60 * 1024 * 1024
        ),
        name="routed",
    )(normed, tab, mid, *weights)


def expert_rows(arrived, gate_w, up_w, down_w):
    width = arrived.shape[-1]
    flat_rows = arrived.reshape(-1, width)
    gate = jnp.dot(flat_rows, gate_w, preferred_element_type=jnp.float32)
    upper = jnp.dot(flat_rows, up_w, preferred_element_type=jnp.float32)
    expert_hidden = (jax.nn.silu(gate) * upper).astype(jnp.bfloat16)
    result = jnp.dot(expert_hidden, down_w, preferred_element_type=jnp.float32).astype(jnp.bfloat16)
    return result.reshape(arrived.shape[:-1] + (result.shape[-1],))


def shards(
    queries,
    keys_values,
    doc_ids,
    head_sink,
    out_weight,
    hidden_in,
    norm_gain,
    expert_gate,
    expert_up,
    expert_down,
    routes,
    route_weight,
):
    tok_here = queries.shape[0]
    heads_here = head_sink.shape[0]
    kv_here = keys_values.shape[1]
    group = heads_here // kv_here
    head_dim = keys_values.shape[2] // 2
    docs_wide = jnp.broadcast_to(
        doc_ids.astype(jnp.bfloat16)[:, None], (tok_here, keys_values.shape[2])
    )
    slab = jnp.concatenate([keys_values.reshape(tok_here, -1), docs_wide], axis=1)
    slab = with_halo(slab, "sp", WIN)
    kv_ext = slab[:, : kv_here * keys_values.shape[2]].reshape(
        -1, kv_here, keys_values.shape[2]
    )
    docs_ext = slab[:, kv_here * keys_values.shape[2]].astype(jnp.int32)
    offset = lax.axis_index("sp") * tok_here
    seq_total = lax.axis_size("sp") * tok_here
    span_rows = min(512, tok_here)
    sink_logit = head_sink.reshape(kv_here, group)[:, :, None, None]

    def one_span(span_index):
        first_row = span_index * span_rows
        q_span = queries.reshape(span_rows, kv_here, group, head_dim)
        scores = jnp.einsum(
            "qhgd,khd->hgqk", q_span, kv_ext[..., :head_dim], preferred_element_type=jnp.float32
        ) * HD ** (-0.5)
        query_pos = offset + first_row + jnp.arange(span_rows, dtype=jnp.int32)
        key_pos = offset + first_row - WIN + jnp.arange(span_rows + 2 * WIN, dtype=jnp.int32)
        inside = (key_pos >= 0) & (key_pos < seq_total)
        allowed = (
            (jnp.abs(key_pos[None, :] - query_pos[:, None]) <= WIN)
            & inside[None, :]
            & (docs_ext[None, :] == doc_ids[:, None])
        )
        masked = jnp.where(allowed, scores, -1e30)
        row_max = jnp.maximum(masked.max(-1, keepdims=True), sink_logit)
        exp_scores = jnp.where(allowed, jnp.exp(masked - row_max), 0.0)
        total_mass = exp_scores.sum(-1, keepdims=True) + jnp.exp(sink_logit - row_max)
        weights = (exp_scores / total_mass).astype(jnp.bfloat16)
        outcome = jnp.einsum(
            "hgqk,khd->qhgd", weights, kv_ext[..., head_dim:], preferred_element_type=jnp.float32
        )
        return outcome.astype(jnp.bfloat16).reshape(span_rows, heads_here * head_dim)

    attended = lax.map(one_span, jnp.arange(tok_here // span_rows, dtype=jnp.int32)).reshape(
        tok_here, -1
    )
    if lax.axis_size("tp") == 2:
        tp = lax.axis_index("tp")
        half = tok_here // 2
        mine = lax.dynamic_slice_in_dim(attended, tp * half, half, 0)
        other = lax.ppermute(
            lax.dynamic_slice_in_dim(attended, (1 - tp) * half, half, 0), "tp", [(0, 1), (1, 0)]
        )
        gathered = jnp.concatenate(
            [jnp.where(tp == 0, mine, other), jnp.where(tp == 0, other, mine)], axis=1
        )
    else:
        gathered = lax.all_to_all(attended, "tp", split_axis=0, concat_axis=1, tiled=True)
    projected = jnp.dot(gathered, out_weight, preferred_element_type=jnp.float32)
    mid_wide = (hidden_in.astype(jnp.float32) + projected).astype(jnp.bfloat16).astype(jnp.float32)
    normed = (
        mid_wide
        * lax.rsqrt(jnp.mean(mid_wide * mid_wide, axis=-1, keepdims=True) + 1e-06)
        * norm_gain
    ).astype(jnp.bfloat16)
    local_rows = normed.shape[0]
    topk = routes.shape[1]
    width = normed.shape[1]
    sp_count = lax.axis_size("sp")
    tp_count = lax.axis_size("tp")
    expert_count = sp_count * tp_count
    capacity = 2 * local_rows * topk // expert_count
    flat_routes = routes.reshape(-1)
    one_hot = (flat_routes[:, None] == jnp.arange(expert_count, dtype=jnp.int32)[None, :]).astype(
        jnp.int32
    )
    slot_rank = (jnp.cumsum(one_hot, axis=0) * one_hot).sum(-1) - 1
    slot_index = flat_routes * capacity + slot_rank
    if capacity % 16 == 0 and sp_count % PLANES == 0 and topk == 2:
        tab = jnp.concatenate(
            [
                slot_index.reshape(local_rows, topk).astype(jnp.float32).T,
                route_weight.T,
                jnp.zeros((4, local_rows), jnp.float32),
            ],
            axis=0,
        )
        return routed_by_plane(
            normed,
            mid_wide.astype(jnp.bfloat16),
            tab,
            PLANES,
            capacity,
            (expert_gate[0], expert_up[0], expert_down[0]),
        )
    repeated = jnp.repeat(normed, topk, axis=0)
    buffer_rows = (
        jnp.zeros((expert_count * capacity, width), jnp.bfloat16).at[slot_index].set(repeated)
    )
    sent = buffer_rows.reshape(expert_count, capacity, width)
    finished = expert_rows(
        lax.all_to_all(sent, ("sp", "tp"), split_axis=0, concat_axis=0, tiled=True),
        expert_gate[0],
        expert_up[0],
        expert_down[0],
    )
    returned = lax.all_to_all(finished, ("sp", "tp"), split_axis=0, concat_axis=0, tiled=True)
    returned = returned.reshape(expert_count * capacity, width)
    picked = returned[slot_index].astype(jnp.float32).reshape(local_rows, topk, width)
    mixture = jnp.sum(picked * route_weight[..., None], axis=1)
    return (mid_wide + mixture).astype(jnp.bfloat16)


def solution(mesh):
    placed = (
        P("sp", "tp"),
        P("sp", "tp", None),
        P("sp"),
        P("tp"),
        P(),
        P(("sp", "tp"), None),
        P(),
        P(("sp", "tp"), None, None),
        P(("sp", "tp"), None, None),
        P(("sp", "tp"), None, None),
        P(("sp", "tp"), None),
        P(("sp", "tp"), None),
    )
    return jax.shard_map(
        shards, mesh=mesh, in_specs=placed, out_specs=P(("sp", "tp"), None), check_vma=False
    )
```

```python
import functools

import jax
import jax.numpy as jnp
from jax import lax
from jax.experimental import pallas as pl
from jax.experimental.pallas import tpu as pltpu
from jax.sharding import PartitionSpec as P

HD = 64
LANES = 128
WIN = 128
PLANES = 4
CUTS = 8
TILE = 256
LAND_LAG = 2
HELD_LAG = 2
FAR_LAG = 2
MESH = pl.DeviceIdType.MESH


def with_halo(cells, axis, width):
    count = lax.axis_size(axis)
    ends = count - 1
    return jnp.concatenate(
        [
            lax.ppermute(cells[-width:], axis, [(i, (i + 1) % count) for i in range(ends)]),
            cells,
            lax.ppermute(cells[:width], axis, [((i + 1) % count, i) for i in range(ends)]),
        ],
        axis=0,
    )


def place(stride, tps):
    sp = lax.axis_index("sp")
    tp = lax.axis_index("tp")
    return lax.div(sp, stride), lax.rem(sp, stride), tp, lax.rem(sp, stride) * tps + tp


def greet(z, r, tp, p, planes, stride, tps):
    peers = stride * tps
    barrier = pltpu.get_barrier_semaphore()
    for k in range(1, peers):
        pd = lax.rem(p + k, peers)
        pl.semaphore_signal(
            barrier,
            inc=1,
            device_id=(z * stride + lax.div(pd, tps), lax.rem(pd, tps)),
            device_id_type=MESH,
        )

    @pl.when(z > 0)
    def _():
        pl.semaphore_signal(
            barrier, inc=1, device_id=((z - 1) * stride + r, tp), device_id_type=MESH
        )

    @pl.when(z < planes - 1)
    def _():
        pl.semaphore_signal(
            barrier, inc=1, device_id=((z + 1) * stride + r, tp), device_id_type=MESH
        )

    first = (z > 0) & (r == 0)
    last = (z < planes - 1) & (r == stride - 1)

    @pl.when(first)
    def _():
        pl.semaphore_signal(
            barrier, inc=1, device_id=(z * stride - 1, tp), device_id_type=MESH
        )

    @pl.when(last)
    def _():
        pl.semaphore_signal(
            barrier, inc=1, device_id=((z + 1) * stride, tp), device_id_type=MESH
        )

    count = peers - 1
    for there in (z > 0, z < planes - 1, first, last):
        count = count + there.astype(jnp.int32)
    pl.semaphore_wait(barrier, count)


def slot_hits(tab, z, slots, rows):
    ids = lax.broadcasted_iota(jnp.int32, (slots, rows), 0) + z * slots
    ids = ids.astype(jnp.float32)
    return ids == tab[0:1, :], ids == tab[1:2, :]


def layer_kernel(
    planes, stride, tps, cap,
    q_ref, slab_ref, sink_ref, gain_ref, routes_ref, share_ref,
    out_w_ref, hidden_in_ref, gate_ref, up_ref, down_ref, out_ref,
    reach, outbox, gathered, out_w, resid, bias, squares,
    toks, stage, land, results, held, part, from_low, from_high,
    gate_w, up_w, down_w, gate_sum, up_sum, hidden, mixer, total, tabs,
    zsend, zrecv, psend, precv, rsend, rrecv, csend, lowrecv, highrecv, tsend, trecv, wsem,
    hsend, hrecv, xsend, xrecv, ssem,
):
    z, r, tp, p = place(stride, tps)
    peers = stride * tps
    rows, width = out_ref.shape
    cols = width // CUTS
    slots = peers * cap
    near = planes - 1
    packed = planes * CUTS
    sp = z * stride + r
    ends = planes * stride - 1
    tok_here, heads_wide = q_ref.shape
    kv_wide = slab_ref.shape[1] - LANES
    starts = [
        pltpu.make_async_copy(source, target, ssem.at[k])
        for k, (source, target) in enumerate([(out_w_ref, out_w), (hidden_in_ref, resid)])
    ]
    loads = [
        pltpu.make_async_copy(source, target, wsem.at[k])
        for k, (source, target) in enumerate(
            [(gate_ref, gate_w), (up_ref, up_w), (down_ref, down_w)]
        )
    ]
    for load in starts:
        load.start()
    greet(z, r, tp, p, planes, stride, tps)

    def halo(side):
        there = 0 if side else tok_here + WIN
        return pltpu.make_async_remote_copy(
            src_ref=slab_ref.at[pl.ds((tok_here - WIN) * side, WIN), :],
            dst_ref=reach.at[pl.ds(there, WIN), :],
            send_sem=hsend.at[side],
            recv_sem=hrecv.at[side],
            device_id=(sp - 1 + 2 * side, tp),
            device_id_type=MESH,
        )

    def swap(k, at):
        return pltpu.make_async_remote_copy(
            src_ref=outbox.at[k],
            dst_ref=gathered.at[
                pl.ds(pl.multiple_of(at * WIN, WIN), WIN),
                pl.ds(pl.multiple_of(tp * heads_wide, LANES), heads_wide),
            ],
            send_sem=xsend.at[k],
            recv_sem=xrecv.at[k],
            device_id=(sp, 1 - tp),
            device_id_type=MESH,
        )

    for side in range(2):

        @pl.when((sp < ends) if side else (sp > 0))
        def _():
            halo(side).start()

    for load in loads:
        load.start()

    @pl.when(sp == 0)
    def _():
        reach[0:WIN, :] = jnp.zeros((WIN, reach.shape[1]), reach.dtype)

    @pl.when(sp == ends)
    def _():
        reach[tok_here + WIN :, :] = jnp.zeros((WIN, reach.shape[1]), reach.dtype)

    reach[WIN : tok_here + WIN, :] = slab_ref[...]
    picks = routes_ref[...]
    expert = lax.broadcasted_iota(jnp.int32, (planes * peers, rows), 0)
    early = lax.broadcasted_iota(jnp.int32, (rows, rows), 0) < lax.broadcasted_iota(
        jnp.int32, (rows, rows), 1
    )
    chosen = [jnp.where(expert == picks[k : k + 1, :], 1.0, 0.0) for k in range(2)]
    ahead = jnp.dot(
        (chosen[0] + chosen[1]).astype(jnp.bfloat16),
        jnp.where(early, 1.0, 0.0).astype(jnp.bfloat16),
        preferred_element_type=jnp.float32,
    )
    for k in range(2):
        place_in = jnp.sum(chosen[k] * ahead, axis=0, keepdims=True)
        tabs[z, k : k + 1, :] = picks[k : k + 1, :].astype(jnp.float32) * cap + place_in
        tabs[z, k + 2 : k + 3, :] = share_ref[k : k + 1, :]
    tabs[z, 4:8, :] = jnp.zeros((4, rows), jnp.float32)

    halves = rows // WIN
    span_keys = 3 * WIN
    nt = (((1,), (1,)), ((), ()))

    def attend(b, out_at):
        near_rows = pl.ds(pl.multiple_of(b * WIN, WIN), WIN)
        window = pl.ds(pl.multiple_of(b * WIN, WIN), span_keys)
        middle = pl.ds(pl.multiple_of(b * WIN + WIN, WIN), WIN)
        same = lax.dot_general(
            reach[middle, kv_wide:], reach[window, kv_wide:], nt,
            preferred_element_type=jnp.float32,
        )
        i = lax.broadcasted_iota(jnp.int32, (WIN, span_keys), 0)
        j = lax.broadcasted_iota(jnp.int32, (WIN, span_keys), 1)
        bias[...] = jnp.where((j >= i) & (j <= i + 2 * WIN) & (same > 0.5), 0.0, -1e30)
        low_keys = lax.broadcasted_iota(jnp.int32, (span_keys, LANES), 1) < HD
        low = lax.broadcasted_iota(jnp.int32, (WIN, LANES), 1) < HD
        pairs = heads_wide // kv_wide
        for g in range(kv_wide // LANES):
            both = reach[window, g * LANES : (g + 1) * LANES].astype(jnp.float32)
            turned = pltpu.roll(both, HD, 1)
            keys = [
                jnp.where(low_keys, both, 0.0).astype(jnp.bfloat16),
                jnp.where(low_keys, 0.0, turned).astype(jnp.bfloat16),
            ]
            values = jnp.concatenate(
                [
                    jnp.where(low_keys, turned, both).astype(jnp.bfloat16),
                    jnp.ones((span_keys, LANES), jnp.bfloat16),
                ],
                axis=1,
            )
            for pair in range(pairs):
                at = (g * pairs + pair) * LANES
                query = q_ref[near_rows, at : at + LANES] * jnp.bfloat16(HD**-0.5)
                done = []
                for odd in range(2):
                    sink = sink_ref[(g * pairs + pair) * 2 + odd]
                    score = lax.dot_general(
                        query, keys[odd], nt, preferred_element_type=jnp.float32
                    )
                    score = score + bias[...]
                    row_max = jnp.maximum(jnp.max(score, axis=1, keepdims=True), sink)
                    weight = jnp.exp(score - row_max).astype(jnp.bfloat16)
                    outcome = jnp.dot(weight, values, preferred_element_type=jnp.float32)
                    mass = outcome[:, LANES:] + jnp.exp(sink - row_max)
                    done.append(outcome[:, :LANES] / mass)
                out_at(at)[...] = jnp.where(low, done[0], done[1]).astype(jnp.bfloat16)

    def block_of(k):
        return jnp.where(
            tp == 0,
            jnp.where(k < halves, halves + k, 2 * halves - 1 - k),
            jnp.where(k < halves, halves - 1 - k, k),
        )

    @pl.loop(0, 2 * halves)
    def _(k):
        b = block_of(k)

        @pl.when((b == 0) & (sp > 0))
        def _():
            halo(1).wait_recv()

        @pl.when((b == 2 * halves - 1) & (sp < ends))
        def _():
            halo(0).wait_recv()

        box = jnp.minimum(k, halves)
        attend(b, lambda at: outbox.at[box, :, pl.ds(at, LANES)])

        @pl.when(k < halves)
        def _():
            swap(k, b - halves * (1 - tp)).start()

        @pl.when(k >= halves)
        def _():
            gathered[
                pl.ds(pl.multiple_of((b - halves * tp) * WIN, WIN), WIN),
                pl.ds(pl.multiple_of(tp * heads_wide, LANES), heads_wide),
            ] = outbox[halves]

    for load in starts:
        load.wait()
    squares[...] = jnp.zeros_like(squares)
    for k in range(halves):
        swap(k, 0).wait_recv()

    @pl.loop(0, width // TILE)
    def _(c):
        at = pl.ds(pl.multiple_of(c * TILE, TILE), TILE)
        mid = resid[:, at].astype(jnp.float32) + jnp.dot(
            gathered[...], out_w[:, at], preferred_element_type=jnp.float32
        )
        mid = mid.astype(jnp.bfloat16).astype(jnp.float32)
        total[:, at] = mid
        square = mid * mid
        for k in range(TILE // LANES):
            squares[...] += square[:, k * LANES : (k + 1) * LANES]

    spread = jnp.sum(squares[...], axis=1, keepdims=True) * (1.0 / width)
    scale = lax.rsqrt(spread + 1e-06)

    def block(b):
        inward = jnp.where(z < planes // 2, z + b, z - b)
        outward = jnp.where(z < planes // 2, z - 1, z + 1)
        return jnp.where((inward >= 0) & (inward < planes), inward, outward)

    def span(h):
        return pl.ds(pl.multiple_of(h * cols, cols), cols)

    def seat(k):
        return pl.ds(pl.multiple_of(k * cap, cap), cap)

    def beside(side):
        return ((z + 1 - 2 * side) * stride + r, tp)

    def fellow(k):
        return (z * stride + lax.div(k, tps), lax.rem(k, tps))

    def hop(zs, h, side):
        return pltpu.make_async_remote_copy(
            src_ref=toks.at[zs, :, span(h)],
            dst_ref=toks.at[zs, :, span(h)],
            send_sem=zsend.at[side, zs, h],
            recv_sem=zrecv.at[zs, h],
            device_id=beside(side),
            device_id_type=MESH,
        )

    def tab_hop(zs, side, source):
        return pltpu.make_async_remote_copy(
            src_ref=source,
            dst_ref=tabs.at[zs],
            send_sem=tsend.at[side, zs],
            recv_sem=trecv.at[zs],
            device_id=beside(side),
            device_id_type=MESH,
        )

    def give(zs, h, dest, at):
        return pltpu.make_async_remote_copy(
            src_ref=stage.at[zs, seat(dest), span(h)],
            dst_ref=land.at[zs, seat(at), span(h)],
            send_sem=psend.at[zs, h, dest],
            recv_sem=precv.at[zs, h, at],
            device_id=fellow(dest),
            device_id_type=MESH,
        )

    def back(zs, h, dest, at):
        return pltpu.make_async_remote_copy(
            src_ref=results.at[zs, seat(dest), span(h)],
            dst_ref=held.at[zs, seat(at), span(h)],
            send_sem=rsend.at[zs, h, dest],
            recv_sem=rrecv.at[zs, h, at],
            device_id=fellow(dest),
            device_id_type=MESH,
        )

    def climb(zs, h):
        return pltpu.make_async_remote_copy(
            src_ref=part.at[zs, :, span(h)],
            dst_ref=from_low.at[zs, :, span(h)],
            send_sem=csend.at[zs, h],
            recv_sem=lowrecv.at[zs, h],
            device_id=beside(0),
            device_id_type=MESH,
        )

    def sink(zs, h):
        return pltpu.make_async_remote_copy(
            src_ref=part.at[zs, :, span(h)],
            dst_ref=from_high.at[zs, :, span(h)],
            send_sem=csend.at[zs, h],
            recv_sem=highrecv.at[zs, h],
            device_id=beside(1),
            device_id_type=MESH,
        )

    def pack(zs, h):
        first, second = slot_hits(tabs[zs], z, slots, rows)
        pick = jnp.where(first | second, 1.0, 0.0).astype(jnp.bfloat16)
        picked = jnp.dot(pick, toks[zs, :, span(h)], preferred_element_type=jnp.float32)
        stage[zs, :, span(h)] = picked.astype(jnp.bfloat16)
        for k in range(1, peers):
            give(zs, h, lax.rem(p + k, peers), p).start()
        land[zs, seat(p), span(h)] = stage[zs, seat(p), span(h)]

    def expand(zs, h):
        @pl.when(h == 0)
        def _():
            tab = tabs[zs]
            first, second = slot_hits(tab, z, slots, rows)
            mix = jnp.where(first, tab[2:3, :], 0.0) + jnp.where(second, tab[3:4, :], 0.0)
            mixer[zs] = mix.T.astype(jnp.bfloat16)
            gate_sum[...] = jnp.zeros_like(gate_sum)
            up_sum[...] = jnp.zeros_like(up_sum)

        for k in range(1, peers):
            other = lax.rem(p + k, peers)
            give(zs, h, other, other).wait_recv()

        @pl.loop(0, gate_w.shape[1] // TILE)
        def _(c):
            at = pl.ds(pl.multiple_of(c * TILE, TILE), TILE)
            here = land[zs, :, span(h)]
            gate_sum[:, at] += jnp.dot(
                here, gate_w[span(h), at], preferred_element_type=jnp.float32
            )
            up_sum[:, at] += jnp.dot(here, up_w[span(h), at], preferred_element_type=jnp.float32)

        @pl.when(h == CUTS - 1)
        def _():
            @pl.loop(0, gate_w.shape[1] // TILE)
            def _(c):
                at = pl.ds(pl.multiple_of(c * TILE, TILE), TILE)
                gate = gate_sum[:, at]
                hidden[:, at] = (gate / (1.0 + jnp.exp(-gate)) * up_sum[:, at]).astype(
                    jnp.bfloat16
                )

    def contract(zs, h):
        results[zs, :, span(h)] = jnp.dot(
            hidden[...], down_w[:, span(h)], preferred_element_type=jnp.float32
        ).astype(jnp.bfloat16)

    def send_back(zs, h):
        for k in range(1, peers):
            back(zs, h, lax.rem(p + k, peers), p).start()
        held[zs, seat(p), span(h)] = results[zs, seat(p), span(h)]

    def mixed(zs, h):
        for k in range(1, peers):
            back(zs, h, p, lax.rem(p + k, peers)).wait_recv()
        return jnp.dot(mixer[zs], held[zs, :, span(h)], preferred_element_type=jnp.float32)

    def homeward(f):
        @pl.loop(0, 2)
        def _(k):
            down = (k == 0) == (z >= planes // 2)
            g = f - FAR_LAG * k
            round_of = lax.div(g, CUTS) + 1
            h = lax.rem(g, CUTS)
            zs = jnp.where(down, near - round_of, round_of)
            due = (g >= 0) & (g < near * CUTS)

            @pl.when(due & down & (zs < z))
            def _():
                mine = mixed(zs, h)

                @pl.when(z == near)
                def _():
                    part[zs, :, span(h)] = mine.astype(jnp.bfloat16)

                @pl.when(z < near)
                def _():
                    sink(zs, h).wait_recv()
                    above = from_high[zs, :, span(h)].astype(jnp.float32)
                    part[zs, :, span(h)] = (mine + above).astype(jnp.bfloat16)

                sink(zs, h).start()

            @pl.when(due & jnp.logical_not(down) & (zs > z))
            def _():
                mine = mixed(zs, h)

                @pl.when(z == 0)
                def _():
                    part[zs, :, span(h)] = mine.astype(jnp.bfloat16)

                @pl.when(z > 0)
                def _():
                    climb(zs, h).wait_recv()
                    below = from_low[zs, :, span(h)].astype(jnp.float32)
                    part[zs, :, span(h)] = (mine + below).astype(jnp.bfloat16)

                climb(zs, h).start()

    @pl.when(z < near)
    def _():
        tab_hop(z, 0, tabs.at[z]).start()

    @pl.when(z > 0)
    def _():
        tab_hop(z, 1, tabs.at[z]).start()

    @pl.loop(0, CUTS)
    def _(h):
        at = span(h)
        toks[z, :, at] = (total[:, at] * scale * gain_ref[:, at]).astype(jnp.bfloat16)

        @pl.when(z < near)
        def _():
            hop(z, h, 0).start()

        @pl.when(z > 0)
        def _():
            hop(z, h, 1).start()

    @pl.loop(0, CUTS)
    def _(h):
        pack(z, h)

    for load in loads:
        load.wait()

    def turn(k):
        nth = lax.div(k, CUTS)
        return jnp.where(nth < near, block(nth + 1), z), lax.rem(k, CUTS)

    @pl.loop(0, packed + LAND_LAG + CUTS - 1)
    def _(e):
        dist = lax.div(e, CUTS) + 1
        h = lax.rem(e, CUTS)

        @pl.when(dist <= near)
        def _():
            @pl.loop(0, 2)
            def _(side):
                zs = z - dist + 2 * dist * side
                onward = z + 1 - 2 * side

                @pl.when((zs >= 0) & (zs < planes))
                def _():
                    @pl.when(h == 0)
                    def _():
                        tab_hop(zs, side, tabs.at[zs]).wait_recv()

                        @pl.when((onward >= 0) & (onward < planes))
                        def _():
                            tab_hop(zs, side, tabs.at[zs]).start()

                    hop(zs, h, side).wait_recv()

                    @pl.when((onward >= 0) & (onward < planes))
                    def _():
                        hop(zs, h, side).start()

            pack(block(dist), h)

        g = e - LAND_LAG

        @pl.when((g >= 0) & (g < packed))
        def _():
            expand(*turn(g))

        c = g - CUTS + 1

        @pl.when(c >= 0)
        def _():
            contract(*turn(c))
            send_back(*turn(c))

        homeward(c - HELD_LAG)

    @pl.loop(0, CUTS)
    def _(h):
        total[:, span(h)] += mixed(z, h)

        @pl.when(z > 0)
        def _():
            climb(z, h).wait_recv()
            total[:, span(h)] += from_low[z, :, span(h)].astype(jnp.float32)

        @pl.when(z < near)
        def _():
            sink(z, h).wait_recv()
            total[:, span(h)] += from_high[z, :, span(h)].astype(jnp.float32)

        out_ref[:, span(h)] = total[:, span(h)].astype(jnp.bfloat16)

    @pl.loop(0, planes * CUTS)
    def _(e):
        zs = lax.div(e, CUTS)
        h = lax.rem(e, CUTS)

        @pl.when((zs <= z) & (z < near))
        def _():
            hop(zs, h, 0).wait_send()

        @pl.when((zs >= z) & (z > 0))
        def _():
            hop(zs, h, 1).wait_send()

        @pl.when(zs > z)
        def _():
            climb(zs, h).wait_send()

        @pl.when(zs < z)
        def _():
            sink(zs, h).wait_send()

        for k in range(1, peers):
            give(zs, h, lax.rem(p + k, peers), p).wait_send()
            back(zs, h, lax.rem(p + k, peers), p).wait_send()

        @pl.when(h == 0)
        def _():
            @pl.when((zs <= z) & (z < near))
            def _():
                tab_hop(zs, 0, tabs.at[zs]).wait_send()

            @pl.when((zs >= z) & (z > 0))
            def _():
                tab_hop(zs, 1, tabs.at[zs]).wait_send()

    for k in range(halves):
        swap(k, 0).wait_send()

    for side in range(2):

        @pl.when((sp < ends) if side else (sp > 0))
        def _():
            halo(side).wait_send()


def whole_layer(queries, slab, sinks, gain, routes, shares, out_weight, hidden_in, weights, cap):
    planes = PLANES
    rows, width = hidden_in.shape
    tps = lax.axis_size("tp")
    stride = lax.axis_size("sp") // planes
    peers = stride * tps
    slots = peers * cap
    tok_here, heads_wide = queries.shape
    bf16, f32 = jnp.bfloat16, jnp.float32
    dma = pltpu.SemaphoreType.DMA
    vmem = pl.BlockSpec(memory_space=pltpu.VMEM)
    anywhere = pl.BlockSpec(memory_space=pl.ANY)
    hidden = weights[0].shape[1]
    by_slot = pltpu.VMEM((planes, slots, width), bf16)
    by_row = pltpu.VMEM((planes, rows, width), bf16)
    chunks = dma((planes, CUTS))
    fans = dma((planes, CUTS, peers))
    halves = rows // WIN
    return pl.pallas_call(
        functools.partial(layer_kernel, planes, stride, tps, cap),
        out_shape=jax.ShapeDtypeStruct((rows, width), bf16),
        in_specs=[vmem, vmem, pl.BlockSpec(memory_space=pltpu.SMEM), vmem, vmem, vmem]
        + [anywhere] * 5,
        out_specs=vmem,
        scratch_shapes=[
            pltpu.VMEM((tok_here + 2 * WIN, slab.shape[1]), bf16),
            pltpu.VMEM((halves + 1, WIN, heads_wide), bf16),
            pltpu.VMEM((rows, out_weight.shape[0]), bf16),
            pltpu.VMEM(out_weight.shape, bf16),
            pltpu.VMEM((rows, width), bf16),
            pltpu.VMEM((WIN, 3 * WIN), f32),
            pltpu.VMEM((rows, LANES), f32),
            by_row, by_slot, by_slot, by_slot, by_slot, by_row, by_row, by_row,
            pltpu.VMEM((width, hidden), bf16),
            pltpu.VMEM((width, hidden), bf16),
            pltpu.VMEM((hidden, width), bf16),
            pltpu.VMEM((slots, hidden), f32),
            pltpu.VMEM((slots, hidden), f32),
            pltpu.VMEM((slots, hidden), bf16),
            pltpu.VMEM((planes, rows, slots), bf16),
            pltpu.VMEM((rows, width), f32),
            pltpu.VMEM((planes, 8, rows), f32),
            dma((2, planes, CUTS)), chunks, fans, fans, fans, fans, chunks, chunks, chunks,
            dma((2, planes)), dma((planes,)), dma((3,)),
            dma((2,)), dma((2,)), dma((halves,)), dma((halves,)), dma((2,)),
        ],
        compiler_params=pltpu.CompilerParams(
            collective_id=0, has_side_effects=True, vmem_limit_bytes=63 * 1024 * 1024
        ),
        name="layer",
    )(queries, slab, sinks, gain, routes, shares, out_weight, hidden_in, *weights)


def expert_rows(arrived, gate_w, up_w, down_w):
    width = arrived.shape[-1]
    flat_rows = arrived.reshape(-1, width)
    gate = jnp.dot(flat_rows, gate_w, preferred_element_type=jnp.float32)
    upper = jnp.dot(flat_rows, up_w, preferred_element_type=jnp.float32)
    expert_hidden = (jax.nn.silu(gate) * upper).astype(jnp.bfloat16)
    result = jnp.dot(expert_hidden, down_w, preferred_element_type=jnp.float32).astype(jnp.bfloat16)
    return result.reshape(arrived.shape[:-1] + (result.shape[-1],))


def shards(
    queries,
    keys_values,
    doc_ids,
    head_sink,
    out_weight,
    hidden_in,
    norm_gain,
    expert_gate,
    expert_up,
    expert_down,
    routes,
    route_weight,
):
    tok_here = queries.shape[0]
    heads_here = head_sink.shape[0]
    kv_here = keys_values.shape[1]
    group = heads_here // kv_here
    head_dim = keys_values.shape[2] // 2
    topk = routes.shape[1]
    local_rows, width = hidden_in.shape
    sp_count = lax.axis_size("sp")
    tp_count = lax.axis_size("tp")
    expert_count = sp_count * tp_count
    capacity = 2 * local_rows * topk // expert_count
    if (
        capacity % 16 == 0
        and sp_count % PLANES == 0
        and topk == 2
        and tp_count == 2
        and 2 * head_dim == LANES
        and group % 2 == 0
        and local_rows % WIN == 0
    ):
        hot = doc_ids[:, None] == jnp.arange(LANES, dtype=jnp.int32)[None, :]
        return whole_layer(
            queries,
            jnp.concatenate(
                [keys_values.reshape(tok_here, -1), hot.astype(jnp.bfloat16)], axis=1
            ),
            head_sink,
            norm_gain.reshape(1, width),
            routes.T,
            route_weight.T,
            out_weight,
            hidden_in,
            (expert_gate[0], expert_up[0], expert_down[0]),
            capacity,
        )
    docs_wide = jnp.broadcast_to(
        doc_ids.astype(jnp.bfloat16)[:, None], (tok_here, keys_values.shape[2])
    )
    slab = jnp.concatenate([keys_values.reshape(tok_here, -1), docs_wide], axis=1)
    slab = with_halo(slab, "sp", WIN)
    kv_ext = slab[:, : kv_here * keys_values.shape[2]].reshape(
        -1, kv_here, keys_values.shape[2]
    )
    docs_ext = slab[:, kv_here * keys_values.shape[2]].astype(jnp.int32)
    offset = lax.axis_index("sp") * tok_here
    seq_total = lax.axis_size("sp") * tok_here
    span_rows = min(512, tok_here)
    sink_logit = head_sink.reshape(kv_here, group)[:, :, None, None]

    def one_span(span_index):
        first_row = span_index * span_rows
        q_span = queries.reshape(span_rows, kv_here, group, head_dim)
        scores = jnp.einsum(
            "qhgd,khd->hgqk", q_span, kv_ext[..., :head_dim], preferred_element_type=jnp.float32
        ) * HD ** (-0.5)
        query_pos = offset + first_row + jnp.arange(span_rows, dtype=jnp.int32)
        key_pos = offset + first_row - WIN + jnp.arange(span_rows + 2 * WIN, dtype=jnp.int32)
        inside = (key_pos >= 0) & (key_pos < seq_total)
        allowed = (
            (jnp.abs(key_pos[None, :] - query_pos[:, None]) <= WIN)
            & inside[None, :]
            & (docs_ext[None, :] == doc_ids[:, None])
        )
        masked = jnp.where(allowed, scores, -1e30)
        row_max = jnp.maximum(masked.max(-1, keepdims=True), sink_logit)
        exp_scores = jnp.where(allowed, jnp.exp(masked - row_max), 0.0)
        total_mass = exp_scores.sum(-1, keepdims=True) + jnp.exp(sink_logit - row_max)
        weights = (exp_scores / total_mass).astype(jnp.bfloat16)
        outcome = jnp.einsum(
            "hgqk,khd->qhgd", weights, kv_ext[..., head_dim:], preferred_element_type=jnp.float32
        )
        return outcome.astype(jnp.bfloat16).reshape(span_rows, heads_here * head_dim)

    attended = lax.map(one_span, jnp.arange(tok_here // span_rows, dtype=jnp.int32)).reshape(
        tok_here, -1
    )
    if lax.axis_size("tp") == 2:
        tp = lax.axis_index("tp")
        half = tok_here // 2
        mine = lax.dynamic_slice_in_dim(attended, tp * half, half, 0)
        other = lax.ppermute(
            lax.dynamic_slice_in_dim(attended, (1 - tp) * half, half, 0), "tp", [(0, 1), (1, 0)]
        )
        gathered = jnp.concatenate(
            [jnp.where(tp == 0, mine, other), jnp.where(tp == 0, other, mine)], axis=1
        )
    else:
        gathered = lax.all_to_all(attended, "tp", split_axis=0, concat_axis=1, tiled=True)
    projected = jnp.dot(gathered, out_weight, preferred_element_type=jnp.float32)
    mid_wide = (hidden_in.astype(jnp.float32) + projected).astype(jnp.bfloat16).astype(jnp.float32)
    normed = (
        mid_wide
        * lax.rsqrt(jnp.mean(mid_wide * mid_wide, axis=-1, keepdims=True) + 1e-06)
        * norm_gain
    ).astype(jnp.bfloat16)
    flat_routes = routes.reshape(-1)
    one_hot = (flat_routes[:, None] == jnp.arange(expert_count, dtype=jnp.int32)[None, :]).astype(
        jnp.int32
    )
    slot_rank = (jnp.cumsum(one_hot, axis=0) * one_hot).sum(-1) - 1
    slot_index = flat_routes * capacity + slot_rank
    repeated = jnp.repeat(normed, topk, axis=0)
    buffer_rows = (
        jnp.zeros((expert_count * capacity, width), jnp.bfloat16).at[slot_index].set(repeated)
    )
    sent = buffer_rows.reshape(expert_count, capacity, width)
    finished = expert_rows(
        lax.all_to_all(sent, ("sp", "tp"), split_axis=0, concat_axis=0, tiled=True),
        expert_gate[0],
        expert_up[0],
        expert_down[0],
    )
    returned = lax.all_to_all(finished, ("sp", "tp"), split_axis=0, concat_axis=0, tiled=True)
    returned = returned.reshape(expert_count * capacity, width)
    picked = returned[slot_index].astype(jnp.float32).reshape(local_rows, topk, width)
    mixture = jnp.sum(picked * route_weight[..., None], axis=1)
    return (mid_wide + mixture).astype(jnp.bfloat16)


def solution(mesh):
    placed = (
        P("sp", "tp"),
        P("sp", "tp", None),
        P("sp"),
        P("tp"),
        P(),
        P(("sp", "tp"), None),
        P(),
        P(("sp", "tp"), None, None),
        P(("sp", "tp"), None, None),
        P(("sp", "tp"), None, None),
        P(("sp", "tp"), None),
        P(("sp", "tp"), None),
    )
    return jax.shard_map(
        shards, mesh=mesh, in_specs=placed, out_specs=P(("sp", "tp"), None), check_vma=False
    )
```

```python
import functools

import jax
import jax.numpy as jnp
from jax import lax
from jax.experimental import pallas as pl
from jax.experimental.pallas import tpu as pltpu
from jax.sharding import PartitionSpec as P

HD = 64
LANES = 128
WIN = 128
PLANES = 4
CUTS = 8
CORES = 2
TURNS = CUTS // CORES
TILE = 256
LAND_LAG = 2
HELD_LAG = 2
FAR_LAG = 2
MESH = pl.DeviceIdType.MESH


def with_halo(cells, axis, width):
    count = lax.axis_size(axis)
    ends = count - 1
    return jnp.concatenate(
        [
            lax.ppermute(cells[-width:], axis, [(i, (i + 1) % count) for i in range(ends)]),
            cells,
            lax.ppermute(cells[:width], axis, [((i + 1) % count, i) for i in range(ends)]),
        ],
        axis=0,
    )


def place(stride, tps):
    sp = lax.axis_index("sp")
    tp = lax.axis_index("tp")
    return lax.div(sp, stride), lax.rem(sp, stride), tp, lax.rem(sp, stride) * tps + tp


def greet(z, r, tp, p, planes, stride, tps):
    peers = stride * tps
    barrier = pltpu.get_barrier_semaphore()
    for k in range(1, peers):
        pd = lax.rem(p + k, peers)
        pl.semaphore_signal(
            barrier,
            inc=1,
            device_id=(z * stride + lax.div(pd, tps), lax.rem(pd, tps)),
            device_id_type=MESH,
        )

    @pl.when(z > 0)
    def _():
        pl.semaphore_signal(
            barrier, inc=1, device_id=((z - 1) * stride + r, tp), device_id_type=MESH
        )

    @pl.when(z < planes - 1)
    def _():
        pl.semaphore_signal(
            barrier, inc=1, device_id=((z + 1) * stride + r, tp), device_id_type=MESH
        )

    first = (z > 0) & (r == 0)
    last = (z < planes - 1) & (r == stride - 1)

    @pl.when(first)
    def _():
        pl.semaphore_signal(
            barrier, inc=1, device_id=(z * stride - 1, tp), device_id_type=MESH
        )

    @pl.when(last)
    def _():
        pl.semaphore_signal(
            barrier, inc=1, device_id=((z + 1) * stride, tp), device_id_type=MESH
        )

    count = peers - 1
    for there in (z > 0, z < planes - 1, first, last):
        count = count + there.astype(jnp.int32)
    pl.semaphore_wait(barrier, count)


def slot_hits(tab, z, slots, rows):
    ids = lax.broadcasted_iota(jnp.int32, (slots, rows), 0) + z * slots
    ids = ids.astype(jnp.float32)
    return ids == tab[0:1, :], ids == tab[1:2, :]


def layer_kernel(
    planes, stride, tps, cap,
    q_ref, slab_ref, sink_ref, gain_ref, routes_ref, share_ref,
    out_w_ref, hidden_in_ref, gate_ref, up_ref, down_ref, out_ref,
    reach, outbox, gathered, out_w, resid, bias, squares, lend, lent_mid, leaving, arrived,
    toks, stage, land, results, held, part, from_low, from_high,
    gate_w, up_w, down_w, gate_sum, up_sum, hidden, mixer, total, tabs,
    zsend, zrecv, psend, precv, rsend, rrecv, csend, lowrecv, highrecv, tsend, trecv, wsem,
    hsend, hrecv, xsend, xrecv, ssem, lsend, lrecv, msend, mrecv,
):
    z, r, tp, p = place(stride, tps)
    peers = stride * tps
    rows, width = out_ref.shape
    cols = width // CUTS
    slots = peers * cap
    near = planes - 1
    packed = planes * CUTS
    sp = z * stride + r
    core = lax.rem(r, CORES)
    half = width // CORES
    ends = planes * stride - 1
    tok_here, heads_wide = q_ref.shape
    kv_wide = slab_ref.shape[1] - LANES
    starts = [
        pltpu.make_async_copy(source, target, ssem.at[k])
        for k, (source, target) in enumerate([(out_w_ref, out_w), (hidden_in_ref, resid)])
    ]
    loads = [
        pltpu.make_async_copy(source, target, wsem.at[k])
        for k, (source, target) in enumerate(
            [(gate_ref, gate_w), (up_ref, up_w), (down_ref, down_w)]
        )
    ]
    for load in starts:
        load.start()
    greet(z, r, tp, p, planes, stride, tps)

    def halo(side):
        there = 0 if side else tok_here + WIN
        return pltpu.make_async_remote_copy(
            src_ref=slab_ref.at[pl.ds((tok_here - WIN) * side, WIN), :],
            dst_ref=reach.at[pl.ds(there, WIN), :],
            send_sem=hsend.at[side],
            recv_sem=hrecv.at[side],
            device_id=(sp - 1 + 2 * side, tp),
            device_id_type=MESH,
        )

    def swap(k, at):
        return pltpu.make_async_remote_copy(
            src_ref=outbox.at[k],
            dst_ref=gathered.at[
                pl.ds(pl.multiple_of(at * WIN, WIN), WIN),
                pl.ds(pl.multiple_of(tp * heads_wide, LANES), heads_wide),
            ],
            send_sem=xsend.at[k],
            recv_sem=xrecv.at[k],
            device_id=(sp, 1 - tp),
            device_id_type=MESH,
        )

    for side in range(2):

        @pl.when((sp < ends) if side else (sp > 0))
        def _():
            halo(side).start()

    for load in loads:
        load.start()

    @pl.when(sp == 0)
    def _():
        reach[0:WIN, :] = jnp.zeros((WIN, reach.shape[1]), reach.dtype)

    @pl.when(sp == ends)
    def _():
        reach[tok_here + WIN :, :] = jnp.zeros((WIN, reach.shape[1]), reach.dtype)

    reach[WIN : tok_here + WIN, :] = slab_ref[...]
    picks = routes_ref[...]
    expert = lax.broadcasted_iota(jnp.int32, (planes * peers, rows), 0)
    early = lax.broadcasted_iota(jnp.int32, (rows, rows), 0) < lax.broadcasted_iota(
        jnp.int32, (rows, rows), 1
    )
    chosen = [jnp.where(expert == picks[k : k + 1, :], 1.0, 0.0) for k in range(2)]
    ahead = jnp.dot(
        (chosen[0] + chosen[1]).astype(jnp.bfloat16),
        jnp.where(early, 1.0, 0.0).astype(jnp.bfloat16),
        preferred_element_type=jnp.float32,
    )
    for k in range(2):
        place_in = jnp.sum(chosen[k] * ahead, axis=0, keepdims=True)
        tabs[CORES * z + core, k : k + 1, :] = picks[k : k + 1, :].astype(jnp.float32) * cap + place_in
        tabs[CORES * z + core, k + 2 : k + 3, :] = share_ref[k : k + 1, :]
    tabs[CORES * z + core, 4:8, :] = jnp.zeros((4, rows), jnp.float32)

    halves = rows // WIN
    span_keys = 3 * WIN
    nt = (((1,), (1,)), ((), ()))

    def attend(b, out_at):
        near_rows = pl.ds(pl.multiple_of(b * WIN, WIN), WIN)
        window = pl.ds(pl.multiple_of(b * WIN, WIN), span_keys)
        middle = pl.ds(pl.multiple_of(b * WIN + WIN, WIN), WIN)
        same = lax.dot_general(
            reach[middle, kv_wide:], reach[window, kv_wide:], nt,
            preferred_element_type=jnp.float32,
        )
        i = lax.broadcasted_iota(jnp.int32, (WIN, span_keys), 0)
        j = lax.broadcasted_iota(jnp.int32, (WIN, span_keys), 1)
        bias[...] = jnp.where((j >= i) & (j <= i + 2 * WIN) & (same > 0.5), 0.0, -1e30)
        low_keys = lax.broadcasted_iota(jnp.int32, (span_keys, LANES), 1) < HD
        low = lax.broadcasted_iota(jnp.int32, (WIN, LANES), 1) < HD
        pairs = heads_wide // kv_wide
        for g in range(kv_wide // LANES):
            both = reach[window, g * LANES : (g + 1) * LANES].astype(jnp.float32)
            turned = pltpu.roll(both, HD, 1)
            keys = [
                jnp.where(low_keys, both, 0.0).astype(jnp.bfloat16),
                jnp.where(low_keys, 0.0, turned).astype(jnp.bfloat16),
            ]
            values = jnp.concatenate(
                [
                    jnp.where(low_keys, turned, both).astype(jnp.bfloat16),
                    jnp.ones((span_keys, LANES), jnp.bfloat16),
                ],
                axis=1,
            )
            for pair in range(pairs):
                at = (g * pairs + pair) * LANES
                query = q_ref[near_rows, at : at + LANES] * jnp.bfloat16(HD**-0.5)
                done = []
                for odd in range(2):
                    sink = sink_ref[(g * pairs + pair) * 2 + odd]
                    score = lax.dot_general(
                        query, keys[odd], nt, preferred_element_type=jnp.float32
                    )
                    score = score + bias[...]
                    row_max = jnp.maximum(jnp.max(score, axis=1, keepdims=True), sink)
                    weight = jnp.exp(score - row_max).astype(jnp.bfloat16)
                    outcome = jnp.dot(weight, values, preferred_element_type=jnp.float32)
                    mass = outcome[:, LANES:] + jnp.exp(sink - row_max)
                    done.append(outcome[:, :LANES] / mass)
                out_at(at)[...] = jnp.where(low, done[0], done[1]).astype(jnp.bfloat16)

    def block_of(k):
        return jnp.where(
            tp == 0,
            jnp.where(k < halves, halves + k, 2 * halves - 1 - k),
            jnp.where(k < halves, halves - 1 - k, k),
        )

    @pl.loop(0, 2 * halves)
    def _(k):
        b = block_of(k)

        @pl.when((b == 0) & (sp > 0))
        def _():
            halo(1).wait_recv()

        @pl.when((b == 2 * halves - 1) & (sp < ends))
        def _():
            halo(0).wait_recv()

        box = jnp.minimum(k, halves)
        attend(b, lambda at: outbox.at[box, :, pl.ds(at, LANES)])

        @pl.when(k < halves)
        def _():
            swap(k, b - halves * (1 - tp)).start()

        @pl.when(k >= halves)
        def _():
            gathered[
                pl.ds(pl.multiple_of((b - halves * tp) * WIN, WIN), WIN),
                pl.ds(pl.multiple_of(tp * heads_wide, LANES), heads_wide),
            ] = outbox[halves]

    for load in starts:
        load.wait()
    squares[...] = jnp.zeros_like(squares)
    for k in range(halves):
        swap(k, 0).wait_recv()

    @pl.loop(0, width // TILE)
    def _(c):
        at = pl.ds(pl.multiple_of(c * TILE, TILE), TILE)
        mid = resid[:, at].astype(jnp.float32) + jnp.dot(
            gathered[...], out_w[:, at], preferred_element_type=jnp.float32
        )
        resid[:, at] = mid.astype(jnp.bfloat16)
        mid = resid[:, at].astype(jnp.float32)
        total[:, at] = mid
        square = mid * mid
        for k in range(TILE // LANES):
            squares[...] += square[:, k * LANES : (k + 1) * LANES]

    spread = jnp.sum(squares[...], axis=1, keepdims=True) * (1.0 / width)
    scale = lax.rsqrt(spread + 1e-06)

    def block(b):
        inward = jnp.where(z < planes // 2, z + b, z - b)
        outward = jnp.where(z < planes // 2, z - 1, z + 1)
        return jnp.where((inward >= 0) & (inward < planes), inward, outward)

    def span(h):
        return pl.ds(pl.multiple_of(h * cols, cols), cols)

    def seat(k):
        return pl.ds(pl.multiple_of(k * cap, cap), cap)

    def wide(side, h):
        return pl.ds(pl.multiple_of(side * half + h * cols, cols), cols)

    def chip_of(k):
        return lax.div(k, CORES * tps) * tps + lax.rem(k, tps)

    def core_of(k):
        return lax.rem(lax.div(k, tps), CORES)

    def beside(side):
        return ((z + 1 - 2 * side) * stride + r, tp)

    def fellow(k):
        return (z * stride + lax.div(k, tps), lax.rem(k, tps))

    def hop(zs, h, side):
        return pltpu.make_async_remote_copy(
            src_ref=toks.at[zs, :, span(h)],
            dst_ref=toks.at[zs, :, span(h)],
            send_sem=zsend.at[side, zs],
            recv_sem=zrecv.at[zs, h],
            device_id=beside(side),
            device_id_type=MESH,
        )

    def tab_hop(zs, side):
        return pltpu.make_async_remote_copy(
            src_ref=tabs.at[pl.ds(CORES * zs, CORES)],
            dst_ref=tabs.at[pl.ds(CORES * zs, CORES)],
            send_sem=tsend.at[side, zs],
            recv_sem=trecv.at[zs],
            device_id=beside(side),
            device_id_type=MESH,
        )

    def give(zs, h, dest, at):
        return pltpu.make_async_remote_copy(
            src_ref=stage.at[zs, seat(dest), span(h)],
            dst_ref=land.at[zs, seat(chip_of(at)), wide(core_of(at), h)],
            send_sem=psend.at[zs],
            recv_sem=precv.at[zs, h],
            device_id=fellow(dest),
            device_id_type=MESH,
        )

    def back(zs, h, dest, at):
        return pltpu.make_async_remote_copy(
            src_ref=results.at[zs, seat(chip_of(dest)), wide(core_of(dest), h)],
            dst_ref=held.at[zs, seat(at), span(h)],
            send_sem=rsend.at[zs],
            recv_sem=rrecv.at[zs, h],
            device_id=fellow(dest),
            device_id_type=MESH,
        )

    def tally(held_by, send_sem, recv_sem):
        return pltpu.make_async_remote_copy(
            src_ref=held_by,
            dst_ref=held_by,
            send_sem=send_sem,
            recv_sem=recv_sem,
            device_id=(sp + 1 - CORES * core, tp),
            device_id_type=MESH,
        )

    fan = pl.ds(0, (peers - 1) * cap)

    def to_mate(source, target, which, h):
        return pltpu.make_async_remote_copy(
            src_ref=source,
            dst_ref=target,
            send_sem=lsend.at[which, h],
            recv_sem=lrecv.at[which, h],
            device_id=(sp + 1 - CORES * core, tp),
            device_id_type=MESH,
        )

    def lent(h):
        return to_mate(lend.at[:, span(h)], toks.at[CORES * z + core, :, span(h)], 0, h)

    def lent_rest(h):
        return to_mate(resid.at[:, wide(1 - core, h)], lent_mid.at[:, span(h)], 1, h)

    def settled(h):
        return to_mate(leaving.at[:, span(h)], arrived.at[:, span(h)], 2, h)

    def tab_swap():
        own = tabs.at[CORES * z + core]
        return pltpu.make_async_remote_copy(
            src_ref=own,
            dst_ref=own,
            send_sem=msend,
            recv_sem=mrecv,
            device_id=(sp + 1 - CORES * core, tp),
            device_id_type=MESH,
        )

    def climb(zs, h):
        return pltpu.make_async_remote_copy(
            src_ref=part.at[zs, :, span(h)],
            dst_ref=from_low.at[zs, :, span(h)],
            send_sem=csend.at[zs],
            recv_sem=lowrecv.at[zs, h],
            device_id=beside(0),
            device_id_type=MESH,
        )

    def sink(zs, h):
        return pltpu.make_async_remote_copy(
            src_ref=part.at[zs, :, span(h)],
            dst_ref=from_high.at[zs, :, span(h)],
            send_sem=csend.at[zs],
            recv_sem=highrecv.at[zs, h],
            device_id=beside(1),
            device_id_type=MESH,
        )

    def pack(zs, h):
        first, second = slot_hits(tabs[zs], z, slots, rows)
        pick = jnp.where(first | second, 1.0, 0.0).astype(jnp.bfloat16)
        picked = jnp.dot(pick, toks[zs, :, span(h)], preferred_element_type=jnp.float32)
        stage[zs, :, span(h)] = picked.astype(jnp.bfloat16)
        for k in range(1, peers):
            give(zs, h, lax.rem(p + k, peers), p).start()
        land[zs, seat(chip_of(p)), wide(core, h)] = stage[zs, seat(p), span(h)]

    def expand(zs, h):
        @pl.when(h == 0)
        def _():
            tab = tabs[zs]
            first, second = slot_hits(tab, z, slots, rows)
            mix = jnp.where(first, tab[2:3, :], 0.0) + jnp.where(second, tab[3:4, :], 0.0)
            mixer[zs] = mix.T.astype(jnp.bfloat16)
            gate_sum[...] = jnp.zeros_like(gate_sum)
            up_sum[...] = jnp.zeros_like(up_sum)

        tally(stage.at[zs, fan, span(h)], psend.at[zs], precv.at[zs, h]).wait_recv()

        @pl.loop(0, gate_w.shape[1] // TILE)
        def _(c):
            at = pl.ds(pl.multiple_of(c * TILE, TILE), TILE)
            for side in range(CORES):
                here = land[zs, :, wide(side, h)]
                gate_sum[:, at] += jnp.dot(
                    here, gate_w[wide(side, h), at], preferred_element_type=jnp.float32
                )
                up_sum[:, at] += jnp.dot(
                    here, up_w[wide(side, h), at], preferred_element_type=jnp.float32
                )

        @pl.when(h == TURNS - 1)
        def _():
            @pl.loop(0, gate_w.shape[1] // TILE)
            def _(c):
                at = pl.ds(pl.multiple_of(c * TILE, TILE), TILE)
                gate = gate_sum[:, at]
                hidden[:, at] = (gate / (1.0 + jnp.exp(-gate)) * up_sum[:, at]).astype(
                    jnp.bfloat16
                )

    def contract(zs, h):
        for side in range(CORES):
            results[zs, :, wide(side, h)] = jnp.dot(
                hidden[...], down_w[:, wide(side, h)], preferred_element_type=jnp.float32
            ).astype(jnp.bfloat16)

    def send_back(zs, h):
        for k in range(1, peers):
            back(zs, h, lax.rem(p + k, peers), p).start()
        held[zs, seat(p), span(h)] = results[zs, seat(chip_of(p)), wide(core, h)]

    def mixed(zs, h):
        tally(stage.at[zs, fan, span(h)], rsend.at[zs], rrecv.at[zs, h]).wait_recv()
        return jnp.dot(mixer[zs], held[zs, :, span(h)], preferred_element_type=jnp.float32)

    def homeward(f):
        @pl.loop(0, 2)
        def _(k):
            down = (k == 0) == (z >= planes // 2)
            g = f - FAR_LAG * k
            round_of = lax.div(g, CUTS) + 1
            h = lax.rem(g, TURNS)
            home = jnp.where(down, near - round_of, round_of)
            zs = CORES * home + lax.rem(lax.div(g, TURNS), CORES)
            due = (g >= 0) & (g < near * CUTS)

            @pl.when(due & down & (home < z))
            def _():
                mine = mixed(zs, h)

                @pl.when(z == near)
                def _():
                    part[zs, :, span(h)] = mine.astype(jnp.bfloat16)

                @pl.when(z < near)
                def _():
                    sink(zs, h).wait_recv()
                    above = from_high[zs, :, span(h)].astype(jnp.float32)
                    part[zs, :, span(h)] = (mine + above).astype(jnp.bfloat16)

                sink(zs, h).start()

            @pl.when(due & jnp.logical_not(down) & (home > z))
            def _():
                mine = mixed(zs, h)

                @pl.when(z == 0)
                def _():
                    part[zs, :, span(h)] = mine.astype(jnp.bfloat16)

                @pl.when(z > 0)
                def _():
                    climb(zs, h).wait_recv()
                    below = from_low[zs, :, span(h)].astype(jnp.float32)
                    part[zs, :, span(h)] = (mine + below).astype(jnp.bfloat16)

                climb(zs, h).start()

    tab_swap().start()
    for h in range(TURNS):
        at = wide(1 - core, h)
        lend[:, span(h)] = (total[:, at] * scale * gain_ref[:, at]).astype(jnp.bfloat16)
        lent(h).start()
        lent_rest(h).start()

    @pl.loop(0, TURNS)
    def _(h):
        at = wide(core, h)
        toks[CORES * z + core, :, span(h)] = (total[:, at] * scale * gain_ref[:, at]).astype(
            jnp.bfloat16
        )

    tab_swap().wait_recv()

    @pl.when(z < near)
    def _():
        tab_hop(z, 0).start()

    @pl.when(z > 0)
    def _():
        tab_hop(z, 1).start()

    @pl.loop(0, CUTS)
    def _(k):
        c = lax.div(k, TURNS)
        h = lax.rem(k, TURNS)

        @pl.when(c != core)
        def _():
            lent(h).wait_recv()

        @pl.when(z < near)
        def _():
            hop(CORES * z + c, h, 0).start()

        @pl.when(z > 0)
        def _():
            hop(CORES * z + c, h, 1).start()

        pack(CORES * z + c, h)

    for load in loads:
        load.wait()

    def turn(k):
        nth = lax.div(k, CUTS)
        whose = jnp.where(nth < near, block(nth + 1), z)
        return CORES * whose + lax.rem(lax.div(k, TURNS), CORES), lax.rem(k, TURNS)

    @pl.loop(0, packed + LAND_LAG + TURNS - 1)
    def _(e):
        dist = lax.div(e, CUTS) + 1
        i = lax.rem(e, CUTS)
        c = lax.div(i, TURNS)
        h = lax.rem(i, TURNS)

        @pl.when(dist <= near)
        def _():
            @pl.loop(0, 2)
            def _(side):
                zs = z - dist + 2 * dist * side
                onward = z + 1 - 2 * side

                @pl.when((zs >= 0) & (zs < planes))
                def _():
                    @pl.when(i == 0)
                    def _():
                        tab_hop(zs, side).wait_recv()

                        @pl.when((onward >= 0) & (onward < planes))
                        def _():
                            tab_hop(zs, side).start()

                    hop(CORES * zs + c, h, side).wait_recv()

                    @pl.when((onward >= 0) & (onward < planes))
                    def _():
                        hop(CORES * zs + c, h, side).start()

            pack(CORES * block(dist) + c, h)

        g = e - LAND_LAG

        @pl.when((g >= 0) & (g < packed))
        def _():
            expand(*turn(g))

        made = g - TURNS + 1

        @pl.when(made >= 0)
        def _():
            contract(*turn(made))
            send_back(*turn(made))

        homeward(made - HELD_LAG)

    for h in range(TURNS):
        lent_rest(h).wait_recv()

    @pl.loop(0, CUTS)
    def _(k):
        c = lax.div(k, TURNS)
        h = lax.rem(k, TURNS)
        mine = CORES * z + c
        total[:, span(h)] = mixed(mine, h)

        @pl.when(z > 0)
        def _():
            climb(mine, h).wait_recv()
            total[:, span(h)] += from_low[mine, :, span(h)].astype(jnp.float32)

        @pl.when(z < near)
        def _():
            sink(mine, h).wait_recv()
            total[:, span(h)] += from_high[mine, :, span(h)].astype(jnp.float32)

        @pl.when(c == core)
        def _():
            at = wide(core, h)
            out_ref[:, at] = (resid[:, at].astype(jnp.float32) + total[:, span(h)]).astype(
                jnp.bfloat16
            )

        @pl.when(c != core)
        def _():
            leaving[:, span(h)] = (
                lent_mid[:, span(h)].astype(jnp.float32) + total[:, span(h)]
            ).astype(jnp.bfloat16)
            settled(h).start()

    for h in range(TURNS):
        settled(h).wait_recv()
        out_ref[:, wide(1 - core, h)] = arrived[:, span(h)]

    @pl.loop(0, CORES * planes)
    def _(v):
        zs = lax.div(v, CORES)
        sent = toks.at[v]

        @pl.when((zs <= z) & (z < near))
        def _():
            tally(sent, zsend.at[0, v], zrecv.at[v, 0]).wait_send()

        @pl.when((zs >= z) & (z > 0))
        def _():
            tally(sent, zsend.at[1, v], zrecv.at[v, 0]).wait_send()

        @pl.when(zs != z)
        def _():
            tally(sent, csend.at[v], zrecv.at[v, 0]).wait_send()

        tally(stage.at[v, fan, :], psend.at[v], precv.at[v, 0]).wait_send()
        tally(stage.at[v, fan, :], rsend.at[v], rrecv.at[v, 0]).wait_send()

        @pl.when(lax.rem(v, CORES) == 0)
        def _():
            @pl.when((zs <= z) & (z < near))
            def _():
                tab_hop(zs, 0).wait_send()

            @pl.when((zs >= z) & (z > 0))
            def _():
                tab_hop(zs, 1).wait_send()

    tab_swap().wait_send()
    for h in range(TURNS):
        lent(h).wait_send()
        lent_rest(h).wait_send()
        settled(h).wait_send()

    for k in range(halves):
        swap(k, 0).wait_send()

    for side in range(2):

        @pl.when((sp < ends) if side else (sp > 0))
        def _():
            halo(side).wait_send()


def whole_layer(queries, slab, sinks, gain, routes, shares, out_weight, hidden_in, weights, cap):
    planes = PLANES
    rows, width = hidden_in.shape
    tps = lax.axis_size("tp")
    stride = lax.axis_size("sp") // planes
    peers = stride * tps
    slots = peers * cap
    tok_here, heads_wide = queries.shape
    bf16, f32 = jnp.bfloat16, jnp.float32
    dma = pltpu.SemaphoreType.DMA
    vmem = pl.BlockSpec(memory_space=pltpu.VMEM)
    anywhere = pl.BlockSpec(memory_space=pl.ANY)
    hidden = weights[0].shape[1]
    units = CORES * planes
    half = width // CORES
    by_slot = pltpu.VMEM((units, slots, half), bf16)
    by_chip = pltpu.VMEM((units, slots // CORES, width), bf16)
    by_row = pltpu.VMEM((units, rows, half), bf16)
    chunks = dma((units, TURNS))
    each = dma((units,))
    halves = rows // WIN
    return pl.pallas_call(
        functools.partial(layer_kernel, planes, stride, tps, cap),
        out_shape=jax.ShapeDtypeStruct((rows, width), bf16),
        in_specs=[vmem, vmem, pl.BlockSpec(memory_space=pltpu.SMEM), vmem, vmem, vmem]
        + [anywhere] * 5,
        out_specs=vmem,
        scratch_shapes=[
            pltpu.VMEM((tok_here + 2 * WIN, slab.shape[1]), bf16),
            pltpu.VMEM((halves + 1, WIN, heads_wide), bf16),
            pltpu.VMEM((rows, out_weight.shape[0]), bf16),
            pltpu.VMEM(out_weight.shape, bf16),
            pltpu.VMEM((rows, width), bf16),
            pltpu.VMEM((WIN, 3 * WIN), f32),
            pltpu.VMEM((rows, LANES), f32),
            pltpu.VMEM((rows, half), bf16),
            pltpu.VMEM((rows, half), bf16),
            pltpu.VMEM((rows, half), bf16),
            pltpu.VMEM((rows, half), bf16),
            by_row, by_slot, by_chip, by_chip, by_slot, by_row, by_row, by_row,
            pltpu.VMEM((width, hidden), bf16),
            pltpu.VMEM((width, hidden), bf16),
            pltpu.VMEM((hidden, width), bf16),
            pltpu.VMEM((slots // CORES, hidden), f32),
            pltpu.VMEM((slots // CORES, hidden), f32),
            pltpu.VMEM((slots // CORES, hidden), bf16),
            pltpu.VMEM((units, rows, slots), bf16),
            pltpu.VMEM((rows, width), f32),
            pltpu.VMEM((units, 8, rows), f32),
            dma((2, units)), chunks, each, chunks, each, chunks, each, chunks, chunks,
            dma((2, planes)), dma((planes,)), dma((3,)),
            dma((2,)), dma((2,)), dma((halves,)), dma((halves,)), dma((2,)),
            dma((3, TURNS)), dma((3, TURNS)), dma, dma,
        ],
        compiler_params=pltpu.CompilerParams(
            collective_id=0, has_side_effects=True, vmem_limit_bytes=63 * 1024 * 1024
        ),
        name="layer",
    )(queries, slab, sinks, gain, routes, shares, out_weight, hidden_in, *weights)


def expert_rows(arrived, gate_w, up_w, down_w):
    width = arrived.shape[-1]
    flat_rows = arrived.reshape(-1, width)
    gate = jnp.dot(flat_rows, gate_w, preferred_element_type=jnp.float32)
    upper = jnp.dot(flat_rows, up_w, preferred_element_type=jnp.float32)
    expert_hidden = (jax.nn.silu(gate) * upper).astype(jnp.bfloat16)
    result = jnp.dot(expert_hidden, down_w, preferred_element_type=jnp.float32).astype(jnp.bfloat16)
    return result.reshape(arrived.shape[:-1] + (result.shape[-1],))


def shards(
    queries,
    keys_values,
    doc_ids,
    head_sink,
    out_weight,
    hidden_in,
    norm_gain,
    expert_gate,
    expert_up,
    expert_down,
    routes,
    route_weight,
):
    tok_here = queries.shape[0]
    heads_here = head_sink.shape[0]
    kv_here = keys_values.shape[1]
    group = heads_here // kv_here
    head_dim = keys_values.shape[2] // 2
    topk = routes.shape[1]
    local_rows, width = hidden_in.shape
    sp_count = lax.axis_size("sp")
    tp_count = lax.axis_size("tp")
    expert_count = sp_count * tp_count
    capacity = 2 * local_rows * topk // expert_count
    if (
        capacity % 16 == 0
        and sp_count % PLANES == 0
        and topk == 2
        and tp_count == 2
        and 2 * head_dim == LANES
        and group % 2 == 0
        and local_rows % WIN == 0
        and sp_count // PLANES % CORES == 0
    ):
        hot = doc_ids[:, None] == jnp.arange(LANES, dtype=jnp.int32)[None, :]
        return whole_layer(
            queries,
            jnp.concatenate(
                [keys_values.reshape(tok_here, -1), hot.astype(jnp.bfloat16)], axis=1
            ),
            head_sink,
            norm_gain.reshape(1, width),
            routes.T,
            route_weight.T,
            out_weight,
            hidden_in,
            (expert_gate[0], expert_up[0], expert_down[0]),
            capacity,
        )
    docs_wide = jnp.broadcast_to(
        doc_ids.astype(jnp.bfloat16)[:, None], (tok_here, keys_values.shape[2])
    )
    slab = jnp.concatenate([keys_values.reshape(tok_here, -1), docs_wide], axis=1)
    slab = with_halo(slab, "sp", WIN)
    kv_ext = slab[:, : kv_here * keys_values.shape[2]].reshape(
        -1, kv_here, keys_values.shape[2]
    )
    docs_ext = slab[:, kv_here * keys_values.shape[2]].astype(jnp.int32)
    offset = lax.axis_index("sp") * tok_here
    seq_total = lax.axis_size("sp") * tok_here
    span_rows = min(512, tok_here)
    sink_logit = head_sink.reshape(kv_here, group)[:, :, None, None]

    def one_span(span_index):
        first_row = span_index * span_rows
        q_span = queries.reshape(span_rows, kv_here, group, head_dim)
        scores = jnp.einsum(
            "qhgd,khd->hgqk", q_span, kv_ext[..., :head_dim], preferred_element_type=jnp.float32
        ) * HD ** (-0.5)
        query_pos = offset + first_row + jnp.arange(span_rows, dtype=jnp.int32)
        key_pos = offset + first_row - WIN + jnp.arange(span_rows + 2 * WIN, dtype=jnp.int32)
        inside = (key_pos >= 0) & (key_pos < seq_total)
        allowed = (
            (jnp.abs(key_pos[None, :] - query_pos[:, None]) <= WIN)
            & inside[None, :]
            & (docs_ext[None, :] == doc_ids[:, None])
        )
        masked = jnp.where(allowed, scores, -1e30)
        row_max = jnp.maximum(masked.max(-1, keepdims=True), sink_logit)
        exp_scores = jnp.where(allowed, jnp.exp(masked - row_max), 0.0)
        total_mass = exp_scores.sum(-1, keepdims=True) + jnp.exp(sink_logit - row_max)
        weights = (exp_scores / total_mass).astype(jnp.bfloat16)
        outcome = jnp.einsum(
            "hgqk,khd->qhgd", weights, kv_ext[..., head_dim:], preferred_element_type=jnp.float32
        )
        return outcome.astype(jnp.bfloat16).reshape(span_rows, heads_here * head_dim)

    attended = lax.map(one_span, jnp.arange(tok_here // span_rows, dtype=jnp.int32)).reshape(
        tok_here, -1
    )
    if lax.axis_size("tp") == 2:
        tp = lax.axis_index("tp")
        half = tok_here // 2
        mine = lax.dynamic_slice_in_dim(attended, tp * half, half, 0)
        other = lax.ppermute(
            lax.dynamic_slice_in_dim(attended, (1 - tp) * half, half, 0), "tp", [(0, 1), (1, 0)]
        )
        gathered = jnp.concatenate(
            [jnp.where(tp == 0, mine, other), jnp.where(tp == 0, other, mine)], axis=1
        )
    else:
        gathered = lax.all_to_all(attended, "tp", split_axis=0, concat_axis=1, tiled=True)
    projected = jnp.dot(gathered, out_weight, preferred_element_type=jnp.float32)
    mid_wide = (hidden_in.astype(jnp.float32) + projected).astype(jnp.bfloat16).astype(jnp.float32)
    normed = (
        mid_wide
        * lax.rsqrt(jnp.mean(mid_wide * mid_wide, axis=-1, keepdims=True) + 1e-06)
        * norm_gain
    ).astype(jnp.bfloat16)
    flat_routes = routes.reshape(-1)
    one_hot = (flat_routes[:, None] == jnp.arange(expert_count, dtype=jnp.int32)[None, :]).astype(
        jnp.int32
    )
    slot_rank = (jnp.cumsum(one_hot, axis=0) * one_hot).sum(-1) - 1
    slot_index = flat_routes * capacity + slot_rank
    repeated = jnp.repeat(normed, topk, axis=0)
    buffer_rows = (
        jnp.zeros((expert_count * capacity, width), jnp.bfloat16).at[slot_index].set(repeated)
    )
    sent = buffer_rows.reshape(expert_count, capacity, width)
    finished = expert_rows(
        lax.all_to_all(sent, ("sp", "tp"), split_axis=0, concat_axis=0, tiled=True),
        expert_gate[0],
        expert_up[0],
        expert_down[0],
    )
    returned = lax.all_to_all(finished, ("sp", "tp"), split_axis=0, concat_axis=0, tiled=True)
    returned = returned.reshape(expert_count * capacity, width)
    picked = returned[slot_index].astype(jnp.float32).reshape(local_rows, topk, width)
    mixture = jnp.sum(picked * route_weight[..., None], axis=1)
    return (mid_wide + mixture).astype(jnp.bfloat16)


def solution(mesh):
    placed = (
        P("sp", "tp"),
        P("sp", "tp", None),
        P("sp"),
        P("tp"),
        P(),
        P(("sp", "tp"), None),
        P(),
        P(("sp", "tp"), None, None),
        P(("sp", "tp"), None, None),
        P(("sp", "tp"), None, None),
        P(("sp", "tp"), None),
        P(("sp", "tp"), None),
    )
    return jax.shard_map(
        shards, mesh=mesh, in_specs=placed, out_specs=P(("sp", "tp"), None), check_vma=False
    )
```

```python
import functools

import jax
import jax.numpy as jnp
from jax import lax
from jax.experimental import pallas as pl
from jax.experimental.pallas import tpu as pltpu
from jax.sharding import PartitionSpec as P

HD = 64
LANES = 128
WIN = 128
PLANES = 4
CUTS = 8
CORES = 2
TURNS = CUTS // CORES
TILE = 512
LAND_LAG = 2
HELD_LAG = 2
FAR_LAG = 2
MESH = pl.DeviceIdType.MESH


def with_halo(cells, axis, width):
    count = lax.axis_size(axis)
    ends = count - 1
    return jnp.concatenate(
        [
            lax.ppermute(cells[-width:], axis, [(i, (i + 1) % count) for i in range(ends)]),
            cells,
            lax.ppermute(cells[:width], axis, [((i + 1) % count, i) for i in range(ends)]),
        ],
        axis=0,
    )


def place(stride, tps):
    sp = lax.axis_index("sp")
    tp = lax.axis_index("tp")
    return lax.div(sp, stride), lax.rem(sp, stride), tp, lax.rem(sp, stride) * tps + tp


def greet(z, r, tp, p, planes, stride, tps):
    peers = stride * tps
    barrier = pltpu.get_barrier_semaphore()
    for k in range(1, peers):
        pd = lax.rem(p + k, peers)
        pl.semaphore_signal(
            barrier,
            inc=1,
            device_id=(z * stride + lax.div(pd, tps), lax.rem(pd, tps)),
            device_id_type=MESH,
        )

    @pl.when(z > 0)
    def _():
        pl.semaphore_signal(
            barrier, inc=1, device_id=((z - 1) * stride + r, tp), device_id_type=MESH
        )

    @pl.when(z < planes - 1)
    def _():
        pl.semaphore_signal(
            barrier, inc=1, device_id=((z + 1) * stride + r, tp), device_id_type=MESH
        )

    first = (z > 0) & (r == 0)
    last = (z < planes - 1) & (r == stride - 1)

    @pl.when(first)
    def _():
        pl.semaphore_signal(
            barrier, inc=1, device_id=(z * stride - 1, tp), device_id_type=MESH
        )

    @pl.when(last)
    def _():
        pl.semaphore_signal(
            barrier, inc=1, device_id=((z + 1) * stride, tp), device_id_type=MESH
        )

    count = peers - 1
    for there in (z > 0, z < planes - 1, first, last):
        count = count + there.astype(jnp.int32)
    return lambda: pl.semaphore_wait(barrier, count)


def slot_hits(tab, z, slots, rows):
    ids = lax.broadcasted_iota(jnp.int32, (slots, rows), 0) + z * slots
    ids = ids.astype(jnp.float32)
    return ids == tab[0:1, :], ids == tab[1:2, :]


def layer_kernel(
    planes, stride, tps, cap,
    q_ref, kv_ref, doc_ref, sink_ref, gain_ref, routes_ref, share_ref,
    out_w_ref, hidden_in_ref, gate_ref, up_ref, down_ref, out_ref,
    reach, outbox, gathered, resid, bias, squares, lend, lent_mid, leaving, arrived,
    toks, stage, land, results, held, part, from_low, from_high,
    gate_w, up_w, down_w, gate_sum, up_sum, hidden, mixer, total, tabs,
    zsend, zrecv, psend, precv, rsend, rrecv, csend, lowrecv, highrecv, tsend, trecv, wsem,
    hsend, hrecv, xsend, xrecv, ssem, lsend, lrecv, msend, mrecv,
):
    z, r, tp, p = place(stride, tps)
    peers = stride * tps
    rows, width = out_ref.shape
    cols = width // CUTS
    slots = peers * cap
    near = planes - 1
    packed = planes * CUTS
    sp = z * stride + r
    core = lax.rem(r, CORES)
    half = width // CORES
    ends = planes * stride - 1
    tok_here, heads_wide = q_ref.shape
    kv_wide = kv_ref.shape[1]
    deep = out_w_ref.shape[0] // rows
    starts = [pltpu.make_async_copy(hidden_in_ref, resid, ssem.at[CORES * deep])]
    for k in range(deep):
        for side in range(CORES):
            starts.append(
                pltpu.make_async_copy(
                    out_w_ref.at[k * rows : (k + 1) * rows, side * half : (side + 1) * half],
                    part.at[CORES * k + side],
                    ssem.at[CORES * k + side],
                )
            )
    loads = [
        pltpu.make_async_copy(source, target, wsem.at[k])
        for k, (source, target) in enumerate(
            [(gate_ref, gate_w), (up_ref, up_w), (down_ref, down_w)]
        )
    ]
    for load in starts:
        load.start()
    meet = greet(z, r, tp, p, planes, stride, tps)

    def halo(side):
        there = 0 if side else tok_here + WIN
        return pltpu.make_async_remote_copy(
            src_ref=reach.at[pl.ds(WIN + (tok_here - WIN) * side, WIN), :],
            dst_ref=reach.at[pl.ds(there, WIN), :],
            send_sem=hsend.at[side],
            recv_sem=hrecv.at[side],
            device_id=(sp - 1 + 2 * side, tp),
            device_id_type=MESH,
        )

    def tab_swap():
        own = tabs.at[CORES * z + core]
        return pltpu.make_async_remote_copy(
            src_ref=own,
            dst_ref=own,
            send_sem=msend,
            recv_sem=mrecv,
            device_id=(sp + 1 - CORES * core, tp),
            device_id_type=MESH,
        )

    def swap(k, at):
        return pltpu.make_async_remote_copy(
            src_ref=outbox.at[k],
            dst_ref=gathered.at[
                pl.ds(pl.multiple_of(at * WIN, WIN), WIN),
                pl.ds(pl.multiple_of(tp * heads_wide, LANES), heads_wide),
            ],
            send_sem=xsend.at[k],
            recv_sem=xrecv.at[k],
            device_id=(sp, 1 - tp),
            device_id_type=MESH,
        )

    for load in loads:
        load.start()

    @pl.when(sp == 0)
    def _():
        reach[0:WIN, :] = jnp.zeros((WIN, reach.shape[1]), reach.dtype)

    @pl.when(sp == ends)
    def _():
        reach[tok_here + WIN :, :] = jnp.zeros((WIN, reach.shape[1]), reach.dtype)

    reach[WIN : tok_here + WIN, :kv_wide] = kv_ref[...]
    document = lax.broadcasted_iota(jnp.int32, (LANES, tok_here), 0) == doc_ref[...]
    reach[WIN : tok_here + WIN, kv_wide:] = jnp.where(document, 1.0, 0.0).T.astype(jnp.bfloat16)
    picks = routes_ref[...]
    expert = lax.broadcasted_iota(jnp.int32, (planes * peers, rows), 0)
    early = lax.broadcasted_iota(jnp.int32, (rows, rows), 0) < lax.broadcasted_iota(
        jnp.int32, (rows, rows), 1
    )
    chosen = [jnp.where(expert == picks[k : k + 1, :], 1.0, 0.0) for k in range(2)]
    ahead = jnp.dot(
        (chosen[0] + chosen[1]).astype(jnp.bfloat16),
        jnp.where(early, 1.0, 0.0).astype(jnp.bfloat16),
        preferred_element_type=jnp.float32,
    )
    for k in range(2):
        place_in = jnp.sum(chosen[k] * ahead, axis=0, keepdims=True)
        tabs[CORES * z + core, k : k + 1, :] = picks[k : k + 1, :].astype(jnp.float32) * cap + place_in
        tabs[CORES * z + core, k + 2 : k + 3, :] = share_ref[k : k + 1, :]
    tabs[CORES * z + core, 4:8, :] = jnp.zeros((4, rows), jnp.float32)

    halves = rows // WIN
    span_keys = 3 * WIN
    nt = (((1,), (1,)), ((), ()))

    def attend(b, out_at):
        near_rows = pl.ds(pl.multiple_of(b * WIN, WIN), WIN)
        window = pl.ds(pl.multiple_of(b * WIN, WIN), span_keys)
        middle = pl.ds(pl.multiple_of(b * WIN + WIN, WIN), WIN)
        same = lax.dot_general(
            reach[middle, kv_wide:], reach[window, kv_wide:], nt,
            preferred_element_type=jnp.float32,
        )
        i = lax.broadcasted_iota(jnp.int32, (WIN, span_keys), 0)
        j = lax.broadcasted_iota(jnp.int32, (WIN, span_keys), 1)
        bias[...] = jnp.where((j >= i) & (j <= i + 2 * WIN) & (same > 0.5), 0.0, -1e30)
        low_keys = lax.broadcasted_iota(jnp.int32, (span_keys, LANES), 1) < HD
        low = lax.broadcasted_iota(jnp.int32, (WIN, LANES), 1) < HD
        pairs = heads_wide // kv_wide
        for g in range(kv_wide // LANES):
            both = reach[window, g * LANES : (g + 1) * LANES].astype(jnp.float32)
            turned = pltpu.roll(both, HD, 1)
            keys = [
                jnp.where(low_keys, both, 0.0).astype(jnp.bfloat16),
                jnp.where(low_keys, 0.0, turned).astype(jnp.bfloat16),
            ]
            values = jnp.concatenate(
                [
                    jnp.where(low_keys, turned, both).astype(jnp.bfloat16),
                    jnp.ones((span_keys, LANES), jnp.bfloat16),
                ],
                axis=1,
            )
            for pair in range(pairs):
                at = (g * pairs + pair) * LANES
                query = q_ref[near_rows, at : at + LANES] * jnp.bfloat16(HD**-0.5)
                done = []
                for odd in range(2):
                    sink = sink_ref[(g * pairs + pair) * 2 + odd]
                    score = lax.dot_general(
                        query, keys[odd], nt, preferred_element_type=jnp.float32
                    )
                    score = score + bias[...]
                    row_max = jnp.maximum(jnp.max(score, axis=1, keepdims=True), sink)
                    weight = jnp.exp(score - row_max).astype(jnp.bfloat16)
                    outcome = jnp.dot(weight, values, preferred_element_type=jnp.float32)
                    mass = outcome[:, LANES:] + jnp.exp(sink - row_max)
                    done.append(outcome[:, :LANES] / mass)
                out_at(at)[...] = jnp.where(low, done[0], done[1]).astype(jnp.bfloat16)

    def block_of(k):
        return jnp.where(
            tp == 0,
            jnp.where(k < halves, halves + k, 2 * halves - 1 - k),
            jnp.where(k < halves, halves - 1 - k, k),
        )

    attend(block_of(0), lambda at: outbox.at[0, :, pl.ds(at, LANES)])
    meet()

    for side in range(2):

        @pl.when((sp < ends) if side else (sp > 0))
        def _():
            halo(side).start()

    swap(0, block_of(0) - halves * (1 - tp)).start()
    tab_swap().start()

    @pl.loop(1, 2 * halves)
    def _(k):
        b = block_of(k)

        @pl.when((b == 0) & (sp > 0))
        def _():
            halo(1).wait_recv()

        @pl.when((b == 2 * halves - 1) & (sp < ends))
        def _():
            halo(0).wait_recv()

        box = jnp.minimum(k, halves)
        attend(b, lambda at: outbox.at[box, :, pl.ds(at, LANES)])

        @pl.when(k < halves)
        def _():
            swap(k, b - halves * (1 - tp)).start()

        @pl.when(k >= halves)
        def _():
            gathered[
                pl.ds(pl.multiple_of((b - halves * tp) * WIN, WIN), WIN),
                pl.ds(pl.multiple_of(tp * heads_wide, LANES), heads_wide),
            ] = outbox[halves]

    for load in starts:
        load.wait()
    squares[...] = jnp.zeros_like(squares)
    shared = heads_wide // rows

    def project(side, at, whose):
        made = 0.0
        for k in range(shared):
            row = whose * shared + k
            made += jnp.dot(
                gathered[:, pl.ds(pl.multiple_of(row * rows, rows), rows)],
                part[CORES * row + side, :, at],
                preferred_element_type=jnp.float32,
            )
        return made

    def tile(c):
        side = lax.div(c * TILE, half)
        at = pl.ds(pl.multiple_of(c * TILE, TILE), TILE)
        return side, at, pl.ds(pl.multiple_of(lax.rem(c * TILE, half), TILE), TILE)

    @pl.loop(0, width // TILE)
    def _(c):
        side, at, within = tile(c)
        total[:, at] = resid[:, at].astype(jnp.float32) + project(side, within, tp)

    for k in range(halves):
        swap(k, 0).wait_recv()

    @pl.loop(0, width // TILE)
    def _(c):
        side, at, within = tile(c)
        mid = total[:, at] + project(side, within, 1 - tp)
        resid[:, at] = mid.astype(jnp.bfloat16)
        mid = resid[:, at].astype(jnp.float32)
        total[:, at] = mid
        square = mid * mid
        for k in range(TILE // LANES):
            squares[...] += square[:, k * LANES : (k + 1) * LANES]

    spread = jnp.sum(squares[...], axis=1, keepdims=True) * (1.0 / width)
    scale = lax.rsqrt(spread + 1e-06)

    def block(b):
        inward = jnp.where(z < planes // 2, z + b, z - b)
        outward = jnp.where(z < planes // 2, z - 1, z + 1)
        return jnp.where((inward >= 0) & (inward < planes), inward, outward)

    def span(h):
        return pl.ds(pl.multiple_of(h * cols, cols), cols)

    def seat(k):
        return pl.ds(pl.multiple_of(k * cap, cap), cap)

    def wide(side, h):
        return pl.ds(pl.multiple_of(side * half + h * cols, cols), cols)

    def chip_of(k):
        return lax.div(k, CORES * tps) * tps + lax.rem(k, tps)

    def core_of(k):
        return lax.rem(lax.div(k, tps), CORES)

    def beside(side):
        return ((z + 1 - 2 * side) * stride + r, tp)

    def fellow(k):
        return (z * stride + lax.div(k, tps), lax.rem(k, tps))

    def hop(zs, h, side):
        return pltpu.make_async_remote_copy(
            src_ref=toks.at[zs, :, span(h)],
            dst_ref=toks.at[zs, :, span(h)],
            send_sem=zsend.at[side, zs],
            recv_sem=zrecv.at[zs, h],
            device_id=beside(side),
            device_id_type=MESH,
        )

    def tab_hop(zs, side):
        return pltpu.make_async_remote_copy(
            src_ref=tabs.at[pl.ds(CORES * zs, CORES)],
            dst_ref=tabs.at[pl.ds(CORES * zs, CORES)],
            send_sem=tsend.at[side, zs],
            recv_sem=trecv.at[zs],
            device_id=beside(side),
            device_id_type=MESH,
        )

    def give(zs, h, dest, at):
        return pltpu.make_async_remote_copy(
            src_ref=stage.at[zs, seat(dest), span(h)],
            dst_ref=land.at[zs, seat(chip_of(at)), wide(core_of(at), h)],
            send_sem=psend.at[zs],
            recv_sem=precv.at[zs, h],
            device_id=fellow(dest),
            device_id_type=MESH,
        )

    def back(zs, h, dest, at):
        return pltpu.make_async_remote_copy(
            src_ref=results.at[zs, seat(chip_of(dest)), wide(core_of(dest), h)],
            dst_ref=held.at[zs, seat(at), span(h)],
            send_sem=rsend.at[zs],
            recv_sem=rrecv.at[zs, h],
            device_id=fellow(dest),
            device_id_type=MESH,
        )

    def tally(held_by, send_sem, recv_sem):
        return pltpu.make_async_remote_copy(
            src_ref=held_by,
            dst_ref=held_by,
            send_sem=send_sem,
            recv_sem=recv_sem,
            device_id=(sp + 1 - CORES * core, tp),
            device_id_type=MESH,
        )

    fan = pl.ds(0, (peers - 1) * cap)

    def to_mate(source, target, which, h):
        return pltpu.make_async_remote_copy(
            src_ref=source,
            dst_ref=target,
            send_sem=lsend.at[which, h],
            recv_sem=lrecv.at[which, h],
            device_id=(sp + 1 - CORES * core, tp),
            device_id_type=MESH,
        )

    def lent(h):
        return to_mate(lend.at[:, span(h)], toks.at[CORES * z + core, :, span(h)], 0, h)

    def lent_rest(h):
        return to_mate(resid.at[:, wide(1 - core, h)], lent_mid.at[:, span(h)], 1, h)

    def settled(h):
        return to_mate(leaving.at[:, span(h)], arrived.at[:, span(h)], 2, h)

    def climb(zs, h):
        return pltpu.make_async_remote_copy(
            src_ref=part.at[zs, :, span(h)],
            dst_ref=from_low.at[zs, :, span(h)],
            send_sem=csend.at[zs],
            recv_sem=lowrecv.at[zs, h],
            device_id=beside(0),
            device_id_type=MESH,
        )

    def sink(zs, h):
        return pltpu.make_async_remote_copy(
            src_ref=part.at[zs, :, span(h)],
            dst_ref=from_high.at[zs, :, span(h)],
            send_sem=csend.at[zs],
            recv_sem=highrecv.at[zs, h],
            device_id=beside(1),
            device_id_type=MESH,
        )

    def pack(zs, h):
        first, second = slot_hits(tabs[zs], z, slots, rows)
        pick = jnp.where(first | second, 1.0, 0.0).astype(jnp.bfloat16)
        picked = jnp.dot(pick, toks[zs, :, span(h)], preferred_element_type=jnp.float32)
        stage[zs, :, span(h)] = picked.astype(jnp.bfloat16)
        for k in range(1, peers):
            give(zs, h, lax.rem(p + k, peers), p).start()
        land[zs, seat(chip_of(p)), wide(core, h)] = stage[zs, seat(p), span(h)]

    def expand(zs, h):
        @pl.when(h == 0)
        def _():
            tab = tabs[zs]
            first, second = slot_hits(tab, z, slots, rows)
            mix = jnp.where(first, tab[2:3, :], 0.0) + jnp.where(second, tab[3:4, :], 0.0)
            mixer[zs] = mix.T.astype(jnp.bfloat16)
            gate_sum[...] = jnp.zeros_like(gate_sum)
            up_sum[...] = jnp.zeros_like(up_sum)

        tally(stage.at[zs, fan, span(h)], psend.at[zs], precv.at[zs, h]).wait_recv()

        @pl.loop(0, gate_w.shape[1] // TILE)
        def _(c):
            at = pl.ds(pl.multiple_of(c * TILE, TILE), TILE)
            for side in range(CORES):
                here = land[zs, :, wide(side, h)]
                gate_sum[:, at] += jnp.dot(
                    here, gate_w[wide(side, h), at], preferred_element_type=jnp.float32
                )
                up_sum[:, at] += jnp.dot(
                    here, up_w[wide(side, h), at], preferred_element_type=jnp.float32
                )

        @pl.when(h == TURNS - 1)
        def _():
            @pl.loop(0, gate_w.shape[1] // TILE)
            def _(c):
                at = pl.ds(pl.multiple_of(c * TILE, TILE), TILE)
                gate = gate_sum[:, at]
                hidden[:, at] = (gate / (1.0 + jnp.exp(-gate)) * up_sum[:, at]).astype(
                    jnp.bfloat16
                )

    def contract(zs, h):
        for side in range(CORES):
            results[zs, :, wide(side, h)] = jnp.dot(
                hidden[...], down_w[:, wide(side, h)], preferred_element_type=jnp.float32
            ).astype(jnp.bfloat16)

    def send_back(zs, h):
        for k in range(1, peers):
            back(zs, h, lax.rem(p + k, peers), p).start()
        held[zs, seat(p), span(h)] = results[zs, seat(chip_of(p)), wide(core, h)]

    def mixed(zs, h):
        tally(stage.at[zs, fan, span(h)], rsend.at[zs], rrecv.at[zs, h]).wait_recv()
        return jnp.dot(mixer[zs], held[zs, :, span(h)], preferred_element_type=jnp.float32)

    def homeward(f):
        @pl.loop(0, 2)
        def _(k):
            down = (k == 0) == (z >= planes // 2)
            g = f - FAR_LAG * k
            round_of = lax.div(g, CUTS) + 1
            h = lax.rem(g, TURNS)
            home = jnp.where(down, near - round_of, round_of)
            zs = CORES * home + lax.rem(lax.div(g, TURNS), CORES)
            due = (g >= 0) & (g < near * CUTS)

            @pl.when(due & down & (home < z))
            def _():
                mine = mixed(zs, h)

                @pl.when(z == near)
                def _():
                    part[zs, :, span(h)] = mine.astype(jnp.bfloat16)

                @pl.when(z < near)
                def _():
                    sink(zs, h).wait_recv()
                    above = from_high[zs, :, span(h)].astype(jnp.float32)
                    part[zs, :, span(h)] = (mine + above).astype(jnp.bfloat16)

                sink(zs, h).start()

            @pl.when(due & jnp.logical_not(down) & (home > z))
            def _():
                mine = mixed(zs, h)

                @pl.when(z == 0)
                def _():
                    part[zs, :, span(h)] = mine.astype(jnp.bfloat16)

                @pl.when(z > 0)
                def _():
                    climb(zs, h).wait_recv()
                    below = from_low[zs, :, span(h)].astype(jnp.float32)
                    part[zs, :, span(h)] = (mine + below).astype(jnp.bfloat16)

                climb(zs, h).start()

    for h in range(TURNS):
        at = wide(1 - core, h)
        lend[:, span(h)] = (total[:, at] * scale * gain_ref[:, at]).astype(jnp.bfloat16)
        lent(h).start()
        lent_rest(h).start()

    @pl.loop(0, TURNS)
    def _(h):
        at = wide(core, h)
        toks[CORES * z + core, :, span(h)] = (total[:, at] * scale * gain_ref[:, at]).astype(
            jnp.bfloat16
        )

    tab_swap().wait_recv()

    @pl.when(z < near)
    def _():
        tab_hop(z, 0).start()

    @pl.when(z > 0)
    def _():
        tab_hop(z, 1).start()

    @pl.loop(0, CUTS)
    def _(k):
        c = lax.div(k, TURNS)
        h = lax.rem(k, TURNS)

        @pl.when(c != core)
        def _():
            lent(h).wait_recv()

        @pl.when(z < near)
        def _():
            hop(CORES * z + c, h, 0).start()

        @pl.when(z > 0)
        def _():
            hop(CORES * z + c, h, 1).start()

        pack(CORES * z + c, h)

    for load in loads:
        load.wait()

    def turn(k):
        nth = lax.div(k, CUTS)
        whose = jnp.where(nth < near, block(nth + 1), z)
        return CORES * whose + lax.rem(lax.div(k, TURNS), CORES), lax.rem(k, TURNS)

    @pl.loop(0, packed + LAND_LAG + TURNS - 1)
    def _(e):
        dist = lax.div(e, CUTS) + 1
        i = lax.rem(e, CUTS)
        c = lax.div(i, TURNS)
        h = lax.rem(i, TURNS)

        @pl.when(dist <= near)
        def _():
            @pl.loop(0, 2)
            def _(side):
                zs = z - dist + 2 * dist * side
                onward = z + 1 - 2 * side

                @pl.when((zs >= 0) & (zs < planes))
                def _():
                    @pl.when(i == 0)
                    def _():
                        tab_hop(zs, side).wait_recv()

                        @pl.when((onward >= 0) & (onward < planes))
                        def _():
                            tab_hop(zs, side).start()

                    hop(CORES * zs + c, h, side).wait_recv()

                    @pl.when((onward >= 0) & (onward < planes))
                    def _():
                        hop(CORES * zs + c, h, side).start()

            pack(CORES * block(dist) + c, h)

        g = e - LAND_LAG

        @pl.when((g >= 0) & (g < packed))
        def _():
            expand(*turn(g))

        made = g - TURNS + 1

        @pl.when(made >= 0)
        def _():
            contract(*turn(made))
            send_back(*turn(made))

        homeward(made - HELD_LAG)

    for h in range(TURNS):
        lent_rest(h).wait_recv()

    @pl.loop(0, CUTS)
    def _(k):
        c = lax.div(k, TURNS)
        h = lax.rem(k, TURNS)
        mine = CORES * z + c
        total[:, span(h)] = mixed(mine, h)

        @pl.when(z > 0)
        def _():
            climb(mine, h).wait_recv()
            total[:, span(h)] += from_low[mine, :, span(h)].astype(jnp.float32)

        @pl.when(z < near)
        def _():
            sink(mine, h).wait_recv()
            total[:, span(h)] += from_high[mine, :, span(h)].astype(jnp.float32)

        @pl.when(c == core)
        def _():
            at = wide(core, h)
            out_ref[:, at] = (resid[:, at].astype(jnp.float32) + total[:, span(h)]).astype(
                jnp.bfloat16
            )

        @pl.when(c != core)
        def _():
            leaving[:, span(h)] = (
                lent_mid[:, span(h)].astype(jnp.float32) + total[:, span(h)]
            ).astype(jnp.bfloat16)
            settled(h).start()

    for h in range(TURNS):
        settled(h).wait_recv()
        out_ref[:, wide(1 - core, h)] = arrived[:, span(h)]

    @pl.loop(0, CORES * planes)
    def _(v):
        zs = lax.div(v, CORES)
        sent = toks.at[v]

        @pl.when((zs <= z) & (z < near))
        def _():
            tally(sent, zsend.at[0, v], zrecv.at[v, 0]).wait_send()

        @pl.when((zs >= z) & (z > 0))
        def _():
            tally(sent, zsend.at[1, v], zrecv.at[v, 0]).wait_send()

        @pl.when(zs != z)
        def _():
            tally(sent, csend.at[v], zrecv.at[v, 0]).wait_send()

        tally(stage.at[v, fan, :], psend.at[v], precv.at[v, 0]).wait_send()
        tally(stage.at[v, fan, :], rsend.at[v], rrecv.at[v, 0]).wait_send()

        @pl.when(lax.rem(v, CORES) == 0)
        def _():
            @pl.when((zs <= z) & (z < near))
            def _():
                tab_hop(zs, 0).wait_send()

            @pl.when((zs >= z) & (z > 0))
            def _():
                tab_hop(zs, 1).wait_send()

    tab_swap().wait_send()
    for h in range(TURNS):
        lent(h).wait_send()
        lent_rest(h).wait_send()
        settled(h).wait_send()

    for k in range(halves):
        swap(k, 0).wait_send()

    for side in range(2):

        @pl.when((sp < ends) if side else (sp > 0))
        def _():
            halo(side).wait_send()


def whole_layer(queries, kv, docs, sinks, gain, routes, shares, out_weight, hidden_in, weights, cap):
    planes = PLANES
    rows, width = hidden_in.shape
    tps = lax.axis_size("tp")
    stride = lax.axis_size("sp") // planes
    peers = stride * tps
    slots = peers * cap
    tok_here, heads_wide = queries.shape
    bf16, f32 = jnp.bfloat16, jnp.float32
    dma = pltpu.SemaphoreType.DMA
    vmem = pl.BlockSpec(memory_space=pltpu.VMEM)
    anywhere = pl.BlockSpec(memory_space=pl.ANY)
    hidden = weights[0].shape[1]
    units = CORES * planes
    half = width // CORES
    by_slot = pltpu.VMEM((units, slots, half), bf16)
    by_chip = pltpu.VMEM((units, slots // CORES, width), bf16)
    by_row = pltpu.VMEM((units, rows, half), bf16)
    chunks = dma((units, TURNS))
    each = dma((units,))
    halves = rows // WIN
    return pl.pallas_call(
        functools.partial(layer_kernel, planes, stride, tps, cap),
        out_shape=pltpu.VMEM((rows, width), bf16),
        in_specs=[vmem, vmem, vmem, pl.BlockSpec(memory_space=pltpu.SMEM), vmem, vmem, vmem]
        + [anywhere] * 5,
        out_specs=vmem,
        scratch_shapes=[
            pltpu.VMEM((tok_here + 2 * WIN, kv.shape[1] + LANES), bf16),
            pltpu.VMEM((halves + 1, WIN, heads_wide), bf16),
            pltpu.VMEM((rows, out_weight.shape[0]), bf16),
            pltpu.VMEM((rows, width), bf16),
            pltpu.VMEM((WIN, 3 * WIN), f32),
            pltpu.VMEM((rows, LANES), f32),
            pltpu.VMEM((rows, half), bf16),
            pltpu.VMEM((rows, half), bf16),
            pltpu.VMEM((rows, half), bf16),
            pltpu.VMEM((rows, half), bf16),
            by_row, by_slot, by_chip, by_chip, by_slot, by_row, by_row, by_row,
            pltpu.VMEM((width, hidden), bf16),
            pltpu.VMEM((width, hidden), bf16),
            pltpu.VMEM((hidden, width), bf16),
            pltpu.VMEM((slots // CORES, hidden), f32),
            pltpu.VMEM((slots // CORES, hidden), f32),
            pltpu.VMEM((slots // CORES, hidden), bf16),
            pltpu.VMEM((units, rows, slots), bf16),
            pltpu.VMEM((rows, width), f32),
            pltpu.VMEM((units, 8, rows), f32),
            dma((2, units)), chunks, each, chunks, each, chunks, each, chunks, chunks,
            dma((2, planes)), dma((planes,)), dma((3,)),
            dma((2,)), dma((2,)), dma((halves,)), dma((halves,)), dma((units + 1,)),
            dma((3, TURNS)), dma((3, TURNS)), dma, dma,
        ],
        compiler_params=pltpu.CompilerParams(
            collective_id=0, has_side_effects=True, vmem_limit_bytes=57 * 1024 * 1024
        ),
        name="layer",
    )(queries, kv, docs, sinks, gain, routes, shares, out_weight, hidden_in, *weights)


def expert_rows(arrived, gate_w, up_w, down_w):
    width = arrived.shape[-1]
    flat_rows = arrived.reshape(-1, width)
    gate = jnp.dot(flat_rows, gate_w, preferred_element_type=jnp.float32)
    upper = jnp.dot(flat_rows, up_w, preferred_element_type=jnp.float32)
    expert_hidden = (jax.nn.silu(gate) * upper).astype(jnp.bfloat16)
    result = jnp.dot(expert_hidden, down_w, preferred_element_type=jnp.float32).astype(jnp.bfloat16)
    return result.reshape(arrived.shape[:-1] + (result.shape[-1],))


def shards(
    queries,
    keys_values,
    doc_ids,
    head_sink,
    out_weight,
    hidden_in,
    norm_gain,
    expert_gate,
    expert_up,
    expert_down,
    routes,
    route_weight,
):
    tok_here = queries.shape[0]
    heads_here = head_sink.shape[0]
    kv_here = keys_values.shape[1]
    group = heads_here // kv_here
    head_dim = keys_values.shape[2] // 2
    topk = routes.shape[1]
    local_rows, width = hidden_in.shape
    sp_count = lax.axis_size("sp")
    tp_count = lax.axis_size("tp")
    expert_count = sp_count * tp_count
    capacity = 2 * local_rows * topk // expert_count
    if (
        capacity % 16 == 0
        and sp_count % PLANES == 0
        and topk == 2
        and tp_count == 2
        and 2 * head_dim == LANES
        and group % 2 == 0
        and local_rows % WIN == 0
        and local_rows > WIN
        and out_weight.shape[0] == PLANES * local_rows
        and queries.shape[1] % local_rows == 0
        and sp_count // PLANES % CORES == 0
    ):
        return whole_layer(
            queries,
            keys_values.reshape(tok_here, -1),
            doc_ids.reshape(1, tok_here),
            head_sink,
            norm_gain.reshape(1, width),
            routes.T,
            route_weight.T,
            out_weight,
            hidden_in,
            (expert_gate[0], expert_up[0], expert_down[0]),
            capacity,
        )
    docs_wide = jnp.broadcast_to(
        doc_ids.astype(jnp.bfloat16)[:, None], (tok_here, keys_values.shape[2])
    )
    slab = jnp.concatenate([keys_values.reshape(tok_here, -1), docs_wide], axis=1)
    slab = with_halo(slab, "sp", WIN)
    kv_ext = slab[:, : kv_here * keys_values.shape[2]].reshape(
        -1, kv_here, keys_values.shape[2]
    )
    docs_ext = slab[:, kv_here * keys_values.shape[2]].astype(jnp.int32)
    offset = lax.axis_index("sp") * tok_here
    seq_total = lax.axis_size("sp") * tok_here
    span_rows = min(512, tok_here)
    sink_logit = head_sink.reshape(kv_here, group)[:, :, None, None]

    def one_span(span_index):
        first_row = span_index * span_rows
        q_span = queries.reshape(span_rows, kv_here, group, head_dim)
        scores = jnp.einsum(
            "qhgd,khd->hgqk", q_span, kv_ext[..., :head_dim], preferred_element_type=jnp.float32
        ) * HD ** (-0.5)
        query_pos = offset + first_row + jnp.arange(span_rows, dtype=jnp.int32)
        key_pos = offset + first_row - WIN + jnp.arange(span_rows + 2 * WIN, dtype=jnp.int32)
        inside = (key_pos >= 0) & (key_pos < seq_total)
        allowed = (
            (jnp.abs(key_pos[None, :] - query_pos[:, None]) <= WIN)
            & inside[None, :]
            & (docs_ext[None, :] == doc_ids[:, None])
        )
        masked = jnp.where(allowed, scores, -1e30)
        row_max = jnp.maximum(masked.max(-1, keepdims=True), sink_logit)
        exp_scores = jnp.where(allowed, jnp.exp(masked - row_max), 0.0)
        total_mass = exp_scores.sum(-1, keepdims=True) + jnp.exp(sink_logit - row_max)
        weights = (exp_scores / total_mass).astype(jnp.bfloat16)
        outcome = jnp.einsum(
            "hgqk,khd->qhgd", weights, kv_ext[..., head_dim:], preferred_element_type=jnp.float32
        )
        return outcome.astype(jnp.bfloat16).reshape(span_rows, heads_here * head_dim)

    attended = lax.map(one_span, jnp.arange(tok_here // span_rows, dtype=jnp.int32)).reshape(
        tok_here, -1
    )
    if lax.axis_size("tp") == 2:
        tp = lax.axis_index("tp")
        half = tok_here // 2
        mine = lax.dynamic_slice_in_dim(attended, tp * half, half, 0)
        other = lax.ppermute(
            lax.dynamic_slice_in_dim(attended, (1 - tp) * half, half, 0), "tp", [(0, 1), (1, 0)]
        )
        gathered = jnp.concatenate(
            [jnp.where(tp == 0, mine, other), jnp.where(tp == 0, other, mine)], axis=1
        )
    else:
        gathered = lax.all_to_all(attended, "tp", split_axis=0, concat_axis=1, tiled=True)
    projected = jnp.dot(gathered, out_weight, preferred_element_type=jnp.float32)
    mid_wide = (hidden_in.astype(jnp.float32) + projected).astype(jnp.bfloat16).astype(jnp.float32)
    normed = (
        mid_wide
        * lax.rsqrt(jnp.mean(mid_wide * mid_wide, axis=-1, keepdims=True) + 1e-06)
        * norm_gain
    ).astype(jnp.bfloat16)
    flat_routes = routes.reshape(-1)
    one_hot = (flat_routes[:, None] == jnp.arange(expert_count, dtype=jnp.int32)[None, :]).astype(
        jnp.int32
    )
    slot_rank = (jnp.cumsum(one_hot, axis=0) * one_hot).sum(-1) - 1
    slot_index = flat_routes * capacity + slot_rank
    repeated = jnp.repeat(normed, topk, axis=0)
    buffer_rows = (
        jnp.zeros((expert_count * capacity, width), jnp.bfloat16).at[slot_index].set(repeated)
    )
    sent = buffer_rows.reshape(expert_count, capacity, width)
    finished = expert_rows(
        lax.all_to_all(sent, ("sp", "tp"), split_axis=0, concat_axis=0, tiled=True),
        expert_gate[0],
        expert_up[0],
        expert_down[0],
    )
    returned = lax.all_to_all(finished, ("sp", "tp"), split_axis=0, concat_axis=0, tiled=True)
    returned = returned.reshape(expert_count * capacity, width)
    picked = returned[slot_index].astype(jnp.float32).reshape(local_rows, topk, width)
    mixture = jnp.sum(picked * route_weight[..., None], axis=1)
    return (mid_wide + mixture).astype(jnp.bfloat16)


def solution(mesh):
    placed = (
        P("sp", "tp"),
        P("sp", "tp", None),
        P("sp"),
        P("tp"),
        P(),
        P(("sp", "tp"), None),
        P(),
        P(("sp", "tp"), None, None),
        P(("sp", "tp"), None, None),
        P(("sp", "tp"), None, None),
        P(("sp", "tp"), None),
        P(("sp", "tp"), None),
    )
    return jax.shard_map(
        shards, mesh=mesh, in_specs=placed, out_specs=P(("sp", "tp"), None), check_vma=False
    )
```

```python
import functools

import jax
import jax.numpy as jnp
from jax import lax
from jax.experimental import pallas as pl
from jax.experimental.pallas import tpu as pltpu
from jax.sharding import PartitionSpec as P

HD = 64
LANES = 128
WIN = 128
PLANES = 4
CUTS = 8
CORES = 2
TURNS = CUTS // CORES
TILE = 512
LAND_LAG = 2
HELD_LAG = 2
FAR_LAG = 2
LEAD = 3
MESH = pl.DeviceIdType.MESH


def with_halo(cells, axis, width):
    count = lax.axis_size(axis)
    ends = count - 1
    return jnp.concatenate(
        [
            lax.ppermute(cells[-width:], axis, [(i, (i + 1) % count) for i in range(ends)]),
            cells,
            lax.ppermute(cells[:width], axis, [((i + 1) % count, i) for i in range(ends)]),
        ],
        axis=0,
    )


def place(stride, tps):
    sp = lax.axis_index("sp")
    tp = lax.axis_index("tp")
    return lax.div(sp, stride), lax.rem(sp, stride), tp, lax.rem(sp, stride) * tps + tp


def greet(z, r, tp, p, planes, stride, tps):
    peers = stride * tps
    barrier = pltpu.get_barrier_semaphore()
    for k in range(1, peers):
        pd = lax.rem(p + k, peers)
        pl.semaphore_signal(
            barrier,
            inc=1,
            device_id=(z * stride + lax.div(pd, tps), lax.rem(pd, tps)),
            device_id_type=MESH,
        )

    @pl.when(z > 0)
    def _():
        pl.semaphore_signal(
            barrier, inc=1, device_id=((z - 1) * stride + r, tp), device_id_type=MESH
        )

    @pl.when(z < planes - 1)
    def _():
        pl.semaphore_signal(
            barrier, inc=1, device_id=((z + 1) * stride + r, tp), device_id_type=MESH
        )

    first = (z > 0) & (r == 0)
    last = (z < planes - 1) & (r == stride - 1)

    @pl.when(first)
    def _():
        pl.semaphore_signal(
            barrier, inc=1, device_id=(z * stride - 1, tp), device_id_type=MESH
        )

    @pl.when(last)
    def _():
        pl.semaphore_signal(
            barrier, inc=1, device_id=((z + 1) * stride, tp), device_id_type=MESH
        )

    count = peers - 1
    for there in (z > 0, z < planes - 1, first, last):
        count = count + there.astype(jnp.int32)
    return lambda: pl.semaphore_wait(barrier, count)


def slot_hits(tab, z, slots, rows):
    ids = lax.broadcasted_iota(jnp.int32, (slots, rows), 0) + z * slots
    ids = ids.astype(jnp.float32)
    return ids == tab[0:1, :], ids == tab[1:2, :]


def layer_kernel(
    planes, stride, tps, cap,
    q_ref, kv_ref, doc_ref, sink_ref, gain_ref, routes_ref, share_ref,
    out_w_ref, hidden_in_ref, gate_ref, up_ref, down_ref, out_ref,
    reach, outbox, gathered, resid, bias, squares, lend, lent_mid, leaving, arrived,
    toks, stage, land, results, held, part, from_low, from_high,
    gate_w, up_w, down_w, gate_sum, up_sum, hidden, mixer, total, tabs,
    zsend, zrecv, psend, precv, rsend, rrecv, csend, lowrecv, highrecv, tsend, trecv, wsem,
    hsend, hrecv, xsend, xrecv, ssem, lsend, lrecv, msend, mrecv,
):
    z, r, tp, p = place(stride, tps)
    peers = stride * tps
    rows, width = out_ref.shape
    cols = width // CUTS
    slots = peers * cap
    near = planes - 1
    packed = planes * CUTS
    sp = z * stride + r
    core = lax.rem(r, CORES)
    half = width // CORES
    ends = planes * stride - 1
    tok_here, heads_wide = q_ref.shape
    kv_wide = kv_ref.shape[1]
    deep = out_w_ref.shape[0] // rows
    starts = [pltpu.make_async_copy(hidden_in_ref, resid, ssem.at[CORES * deep])]
    for k in range(deep):
        for side in range(CORES):
            starts.append(
                pltpu.make_async_copy(
                    out_w_ref.at[k * rows : (k + 1) * rows, side * half : (side + 1) * half],
                    part.at[CORES * k + side],
                    ssem.at[CORES * k + side],
                )
            )
    loads = [
        pltpu.make_async_copy(source, target, wsem.at[k])
        for k, (source, target) in enumerate(
            [(gate_ref, gate_w), (up_ref, up_w), (down_ref, down_w)]
        )
    ]
    for load in starts:
        load.start()
    meet = greet(z, r, tp, p, planes, stride, tps)

    def halo(side):
        there = 0 if side else tok_here + WIN
        return pltpu.make_async_remote_copy(
            src_ref=reach.at[pl.ds(WIN + (tok_here - WIN) * side, WIN), :],
            dst_ref=reach.at[pl.ds(there, WIN), :],
            send_sem=hsend.at[side],
            recv_sem=hrecv.at[side],
            device_id=(sp - 1 + 2 * side, tp),
            device_id_type=MESH,
        )

    def tab_swap():
        own = tabs.at[CORES * z + core]
        return pltpu.make_async_remote_copy(
            src_ref=own,
            dst_ref=own,
            send_sem=msend,
            recv_sem=mrecv,
            device_id=(sp + 1 - CORES * core, tp),
            device_id_type=MESH,
        )

    def swap(k, at):
        return pltpu.make_async_remote_copy(
            src_ref=outbox.at[k],
            dst_ref=gathered.at[
                pl.ds(pl.multiple_of(at * WIN, WIN), WIN),
                pl.ds(pl.multiple_of(tp * heads_wide, LANES), heads_wide),
            ],
            send_sem=xsend.at[k],
            recv_sem=xrecv.at[k],
            device_id=(sp, 1 - tp),
            device_id_type=MESH,
        )

    for load in loads:
        load.start()

    @pl.when(sp == 0)
    def _():
        reach[0:WIN, :] = jnp.zeros((WIN, reach.shape[1]), reach.dtype)

    @pl.when(sp == ends)
    def _():
        reach[tok_here + WIN :, :] = jnp.zeros((WIN, reach.shape[1]), reach.dtype)

    reach[WIN : tok_here + WIN, :kv_wide] = kv_ref[...]
    document = lax.broadcasted_iota(jnp.int32, (LANES, tok_here), 0) == doc_ref[...]
    reach[WIN : tok_here + WIN, kv_wide:] = jnp.where(document, 1.0, 0.0).T.astype(jnp.bfloat16)
    picks = routes_ref[...]
    expert = lax.broadcasted_iota(jnp.int32, (planes * peers, rows), 0)
    early = lax.broadcasted_iota(jnp.int32, (rows, rows), 0) < lax.broadcasted_iota(
        jnp.int32, (rows, rows), 1
    )
    chosen = [jnp.where(expert == picks[k : k + 1, :], 1.0, 0.0) for k in range(2)]
    ahead = jnp.dot(
        (chosen[0] + chosen[1]).astype(jnp.bfloat16),
        jnp.where(early, 1.0, 0.0).astype(jnp.bfloat16),
        preferred_element_type=jnp.float32,
    )
    for k in range(2):
        place_in = jnp.sum(chosen[k] * ahead, axis=0, keepdims=True)
        tabs[CORES * z + core, k : k + 1, :] = picks[k : k + 1, :].astype(jnp.float32) * cap + place_in
        tabs[CORES * z + core, k + 2 : k + 3, :] = share_ref[k : k + 1, :]
    tabs[CORES * z + core, 4:8, :] = jnp.zeros((4, rows), jnp.float32)

    halves = rows // WIN
    span_keys = 3 * WIN
    nt = (((1,), (1,)), ((), ()))

    def attend(b, out_at):
        near_rows = pl.ds(pl.multiple_of(b * WIN, WIN), WIN)
        window = pl.ds(pl.multiple_of(b * WIN, WIN), span_keys)
        middle = pl.ds(pl.multiple_of(b * WIN + WIN, WIN), WIN)
        same = lax.dot_general(
            reach[middle, kv_wide:], reach[window, kv_wide:], nt,
            preferred_element_type=jnp.float32,
        )
        i = lax.broadcasted_iota(jnp.int32, (WIN, span_keys), 0)
        j = lax.broadcasted_iota(jnp.int32, (WIN, span_keys), 1)
        bias[...] = jnp.where((j >= i) & (j <= i + 2 * WIN) & (same > 0.5), 0.0, -1e30)
        low_keys = lax.broadcasted_iota(jnp.int32, (span_keys, LANES), 1) < HD
        low = lax.broadcasted_iota(jnp.int32, (WIN, LANES), 1) < HD
        pairs = heads_wide // kv_wide
        for g in range(kv_wide // LANES):
            both = reach[window, g * LANES : (g + 1) * LANES].astype(jnp.float32)
            turned = pltpu.roll(both, HD, 1)
            keys = [
                jnp.where(low_keys, both, 0.0).astype(jnp.bfloat16),
                jnp.where(low_keys, 0.0, turned).astype(jnp.bfloat16),
            ]
            values = jnp.concatenate(
                [
                    jnp.where(low_keys, turned, both).astype(jnp.bfloat16),
                    jnp.ones((span_keys, LANES), jnp.bfloat16),
                ],
                axis=1,
            )
            for pair in range(pairs):
                at = (g * pairs + pair) * LANES
                query = q_ref[near_rows, at : at + LANES] * jnp.bfloat16(HD**-0.5)
                done = []
                for odd in range(2):
                    sink = sink_ref[(g * pairs + pair) * 2 + odd]
                    score = lax.dot_general(
                        query, keys[odd], nt, preferred_element_type=jnp.float32
                    )
                    score = score + bias[...]
                    row_max = jnp.maximum(jnp.max(score, axis=1, keepdims=True), sink)
                    weight = jnp.exp(score - row_max).astype(jnp.bfloat16)
                    outcome = jnp.dot(weight, values, preferred_element_type=jnp.float32)
                    mass = outcome[:, LANES:] + jnp.exp(sink - row_max)
                    done.append(outcome[:, :LANES] / mass)
                out_at(at)[...] = jnp.where(low, done[0], done[1]).astype(jnp.bfloat16)

    def block_of(k):
        return jnp.where(
            tp == 0,
            jnp.where(k < halves, halves + k, 2 * halves - 1 - k),
            jnp.where(k < halves, halves - 1 - k, k),
        )

    attend(block_of(0), lambda at: outbox.at[0, :, pl.ds(at, LANES)])
    meet()

    for side in range(2):

        @pl.when((sp < ends) if side else (sp > 0))
        def _():
            halo(side).start()

    swap(0, block_of(0) - halves * (1 - tp)).start()
    tab_swap().start()

    @pl.loop(1, 2 * halves)
    def _(k):
        b = block_of(k)

        @pl.when((b == 0) & (sp > 0))
        def _():
            halo(1).wait_recv()

        @pl.when((b == 2 * halves - 1) & (sp < ends))
        def _():
            halo(0).wait_recv()

        box = jnp.minimum(k, halves)
        attend(b, lambda at: outbox.at[box, :, pl.ds(at, LANES)])

        @pl.when(k < halves)
        def _():
            swap(k, b - halves * (1 - tp)).start()

        @pl.when(k >= halves)
        def _():
            gathered[
                pl.ds(pl.multiple_of((b - halves * tp) * WIN, WIN), WIN),
                pl.ds(pl.multiple_of(tp * heads_wide, LANES), heads_wide),
            ] = outbox[halves]

    for load in starts:
        load.wait()
    squares[...] = jnp.zeros_like(squares)
    shared = heads_wide // rows

    def project(side, at, whose):
        made = 0.0
        for k in range(shared):
            row = whose * shared + k
            made += jnp.dot(
                gathered[:, pl.ds(pl.multiple_of(row * rows, rows), rows)],
                part[CORES * row + side, :, at],
                preferred_element_type=jnp.float32,
            )
        return made

    def tile(c):
        side = lax.div(c * TILE, half)
        at = pl.ds(pl.multiple_of(c * TILE, TILE), TILE)
        return side, at, pl.ds(pl.multiple_of(lax.rem(c * TILE, half), TILE), TILE)

    @pl.loop(0, width // TILE)
    def _(c):
        side, at, within = tile(c)
        total[:, at] = resid[:, at].astype(jnp.float32) + project(side, within, tp)

    for k in range(halves):
        swap(k, 0).wait_recv()

    @pl.loop(0, width // TILE)
    def _(c):
        side, at, within = tile(c)
        mid = total[:, at] + project(side, within, 1 - tp)
        resid[:, at] = mid.astype(jnp.bfloat16)
        mid = resid[:, at].astype(jnp.float32)
        total[:, at] = mid
        square = mid * mid
        for k in range(TILE // LANES):
            squares[...] += square[:, k * LANES : (k + 1) * LANES]

    spread = jnp.sum(squares[...], axis=1, keepdims=True) * (1.0 / width)
    scale = lax.rsqrt(spread + 1e-06)

    def far_second(b):
        return jnp.where(b == 1, 1, jnp.where(b == 2, near, 2))

    def block(b):
        at_end = (z == 0) | (z == near)
        steps = jnp.where(at_end, far_second(b), jnp.where(b == 1, -1, near + 1 - b))
        return jnp.where(z < planes // 2, z + steps, z - steps)

    def span(h):
        return pl.ds(pl.multiple_of(h * cols, cols), cols)

    def seat(k):
        return pl.ds(pl.multiple_of(k * cap, cap), cap)

    def wide(side, h):
        return pl.ds(pl.multiple_of(side * half + h * cols, cols), cols)

    def chip_of(k):
        return lax.div(k, CORES * tps) * tps + lax.rem(k, tps)

    def core_of(k):
        return lax.rem(lax.div(k, tps), CORES)

    def beside(side):
        return ((z + 1 - 2 * side) * stride + r, tp)

    def fellow(k):
        return (z * stride + lax.div(k, tps), lax.rem(k, tps))

    def hop(zs, h, side):
        return pltpu.make_async_remote_copy(
            src_ref=toks.at[zs, :, span(h)],
            dst_ref=toks.at[zs, :, span(h)],
            send_sem=zsend.at[side, zs],
            recv_sem=zrecv.at[zs, h],
            device_id=beside(side),
            device_id_type=MESH,
        )

    def tab_hop(zs, side):
        return pltpu.make_async_remote_copy(
            src_ref=tabs.at[pl.ds(CORES * zs, CORES)],
            dst_ref=tabs.at[pl.ds(CORES * zs, CORES)],
            send_sem=tsend.at[side, zs],
            recv_sem=trecv.at[zs],
            device_id=beside(side),
            device_id_type=MESH,
        )

    def give(zs, h, dest, at):
        return pltpu.make_async_remote_copy(
            src_ref=stage.at[zs, seat(dest), span(h)],
            dst_ref=land.at[zs, seat(chip_of(at)), wide(core_of(at), h)],
            send_sem=psend.at[zs],
            recv_sem=precv.at[zs, h],
            device_id=fellow(dest),
            device_id_type=MESH,
        )

    def back(zs, h, dest, at):
        return pltpu.make_async_remote_copy(
            src_ref=results.at[zs, seat(chip_of(dest)), wide(core_of(dest), h)],
            dst_ref=held.at[zs, seat(at), span(h)],
            send_sem=rsend.at[zs],
            recv_sem=rrecv.at[zs, h],
            device_id=fellow(dest),
            device_id_type=MESH,
        )

    def tally(held_by, send_sem, recv_sem):
        return pltpu.make_async_remote_copy(
            src_ref=held_by,
            dst_ref=held_by,
            send_sem=send_sem,
            recv_sem=recv_sem,
            device_id=(sp + 1 - CORES * core, tp),
            device_id_type=MESH,
        )

    fan = pl.ds(0, (peers - 1) * cap)

    def to_mate(source, target, which, h):
        return pltpu.make_async_remote_copy(
            src_ref=source,
            dst_ref=target,
            send_sem=lsend.at[which, h],
            recv_sem=lrecv.at[which, h],
            device_id=(sp + 1 - CORES * core, tp),
            device_id_type=MESH,
        )

    def lent(h):
        return to_mate(lend.at[:, span(h)], toks.at[CORES * z + core, :, span(h)], 0, h)

    def lent_rest(h):
        return to_mate(resid.at[:, wide(1 - core, h)], lent_mid.at[:, span(h)], 1, h)

    def settled(h):
        return to_mate(leaving.at[:, span(h)], arrived.at[:, span(h)], 2, h)

    def climb(zs, h):
        return pltpu.make_async_remote_copy(
            src_ref=part.at[zs, :, span(h)],
            dst_ref=from_low.at[zs, :, span(h)],
            send_sem=csend.at[zs],
            recv_sem=lowrecv.at[zs, h],
            device_id=beside(0),
            device_id_type=MESH,
        )

    def sink(zs, h):
        return pltpu.make_async_remote_copy(
            src_ref=part.at[zs, :, span(h)],
            dst_ref=from_high.at[zs, :, span(h)],
            send_sem=csend.at[zs],
            recv_sem=highrecv.at[zs, h],
            device_id=beside(1),
            device_id_type=MESH,
        )

    def pack(zs, h):
        first, second = slot_hits(tabs[zs], z, slots, rows)
        pick = jnp.where(first | second, 1.0, 0.0).astype(jnp.bfloat16)
        picked = jnp.dot(pick, toks[zs, :, span(h)], preferred_element_type=jnp.float32)
        stage[zs, :, span(h)] = picked.astype(jnp.bfloat16)
        for k in range(1, peers):
            give(zs, h, lax.rem(p + k, peers), p).start()
        land[zs, seat(chip_of(p)), wide(core, h)] = stage[zs, seat(p), span(h)]

    def expand(zs, h):
        @pl.when(h == 0)
        def _():
            tab = tabs[zs]
            first, second = slot_hits(tab, z, slots, rows)
            mix = jnp.where(first, tab[2:3, :], 0.0) + jnp.where(second, tab[3:4, :], 0.0)
            mixer[zs] = mix.T.astype(jnp.bfloat16)
            gate_sum[...] = jnp.zeros_like(gate_sum)
            up_sum[...] = jnp.zeros_like(up_sum)

        tally(stage.at[zs, fan, span(h)], psend.at[zs], precv.at[zs, h]).wait_recv()

        @pl.loop(0, gate_w.shape[1] // TILE)
        def _(c):
            at = pl.ds(pl.multiple_of(c * TILE, TILE), TILE)
            for side in range(CORES):
                here = land[zs, :, wide(side, h)]
                gate_sum[:, at] += jnp.dot(
                    here, gate_w[wide(side, h), at], preferred_element_type=jnp.float32
                )
                up_sum[:, at] += jnp.dot(
                    here, up_w[wide(side, h), at], preferred_element_type=jnp.float32
                )

        @pl.when(h == TURNS - 1)
        def _():
            @pl.loop(0, gate_w.shape[1] // TILE)
            def _(c):
                at = pl.ds(pl.multiple_of(c * TILE, TILE), TILE)
                gate = gate_sum[:, at]
                hidden[:, at] = (gate / (1.0 + jnp.exp(-gate)) * up_sum[:, at]).astype(
                    jnp.bfloat16
                )

    def contract(zs, h):
        for side in range(CORES):
            results[zs, :, wide(side, h)] = jnp.dot(
                hidden[...], down_w[:, wide(side, h)], preferred_element_type=jnp.float32
            ).astype(jnp.bfloat16)

    def send_back(zs, h):
        for k in range(1, peers):
            back(zs, h, lax.rem(p + k, peers), p).start()
        held[zs, seat(p), span(h)] = results[zs, seat(chip_of(p)), wide(core, h)]

    def mixed(zs, h):
        tally(stage.at[zs, fan, span(h)], rsend.at[zs], rrecv.at[zs, h]).wait_recv()
        return jnp.dot(mixer[zs], held[zs, :, span(h)], preferred_element_type=jnp.float32)

    def homeward(f):
        @pl.loop(0, 2)
        def _(k):
            down = (k == 0) == (z >= planes // 2)
            g = f - FAR_LAG * k
            round_of = lax.div(g, CUTS) + 1
            h = lax.rem(g, TURNS)
            upper = far_second(round_of)
            home = jnp.where(down, near - upper, upper)
            zs = CORES * home + lax.rem(lax.div(g, TURNS), CORES)
            due = (g >= 0) & (g < near * CUTS)

            @pl.when(due & down & (home < z))
            def _():
                mine = mixed(zs, h)

                @pl.when(z == near)
                def _():
                    part[zs, :, span(h)] = mine.astype(jnp.bfloat16)

                @pl.when(z < near)
                def _():
                    sink(zs, h).wait_recv()
                    above = from_high[zs, :, span(h)].astype(jnp.float32)
                    part[zs, :, span(h)] = (mine + above).astype(jnp.bfloat16)

                sink(zs, h).start()

            @pl.when(due & jnp.logical_not(down) & (home > z))
            def _():
                mine = mixed(zs, h)

                @pl.when(z == 0)
                def _():
                    part[zs, :, span(h)] = mine.astype(jnp.bfloat16)

                @pl.when(z > 0)
                def _():
                    climb(zs, h).wait_recv()
                    below = from_low[zs, :, span(h)].astype(jnp.float32)
                    part[zs, :, span(h)] = (mine + below).astype(jnp.bfloat16)

                climb(zs, h).start()

    for h in range(TURNS):
        at = wide(1 - core, h)
        lend[:, span(h)] = (total[:, at] * scale * gain_ref[:, at]).astype(jnp.bfloat16)
        lent(h).start()
        lent_rest(h).start()

    @pl.loop(0, TURNS)
    def _(h):
        at = wide(core, h)
        toks[CORES * z + core, :, span(h)] = (total[:, at] * scale * gain_ref[:, at]).astype(
            jnp.bfloat16
        )

    tab_swap().wait_recv()

    @pl.when(z < near)
    def _():
        tab_hop(z, 0).start()

    @pl.when(z > 0)
    def _():
        tab_hop(z, 1).start()

    @pl.loop(0, CUTS)
    def _(k):
        c = lax.div(k, TURNS)
        h = lax.rem(k, TURNS)

        @pl.when(c != core)
        def _():
            lent(h).wait_recv()

        @pl.when((z < near) & ((z != 1) | (k < LEAD)))
        def _():
            hop(CORES * z + c, h, 0).start()

        @pl.when((z > 0) & ((near - z != 1) | (k < LEAD)))
        def _():
            hop(CORES * z + c, h, 1).start()

        pack(CORES * z + c, h)

    for load in loads:
        load.wait()

    def turn(k):
        nth = lax.div(k, CUTS)
        whose = jnp.where(nth < near, block(nth + 1), z)
        return CORES * whose + lax.rem(lax.div(k, TURNS), CORES), lax.rem(k, TURNS)

    @pl.loop(0, packed + LAND_LAG + TURNS - 1)
    def _(e):
        dist = lax.div(e, CUTS) + 1
        i = lax.rem(e, CUTS)
        c = lax.div(i, TURNS)
        h = lax.rem(i, TURNS)

        @pl.when(dist <= near)
        def _():
            @pl.loop(0, 2)
            def _(side):
                sources = jnp.where(side == 0, z, near - z)
                second = (e >= LEAD) & (e < LEAD + CUTS)
                when_two = jnp.where(second, 2, 1)
                steps = jnp.where(
                    sources == 1, 1, jnp.where(sources == 2, when_two, far_second(dist))
                )
                turn_two = jnp.where(e < LEAD, e, jnp.where(second, e - LEAD, e - CUTS))
                piece = jnp.where(sources == 2, turn_two, i)
                zs = z - steps + 2 * steps * side
                onward = z + 1 - 2 * side
                goes_on = (onward >= 0) & (onward < planes)
                unit = CORES * zs + lax.div(piece, TURNS)
                part_of = lax.rem(piece, TURNS)

                @pl.when(e < sources * CUTS)
                def _():
                    @pl.when(piece == 0)
                    def _():
                        tab_hop(zs, side).wait_recv()

                        @pl.when(goes_on)
                        def _():
                            tab_hop(zs, side).start()

                    hop(unit, part_of, side).wait_recv()

                    @pl.when(goes_on & (sources == 2) & (e == LEAD + CUTS))
                    def _():
                        for k in range(LEAD):
                            hop(CORES * zs + k // TURNS, k % TURNS, side).start()

                    @pl.when(goes_on & ((sources != 2) | (e >= LEAD)))
                    def _():
                        hop(unit, part_of, side).start()

                    @pl.when(goes_on & (sources == 1) & (e == CUTS - 1))
                    def _():
                        for k in range(LEAD, CUTS):
                            hop(CORES * z + k // TURNS, k % TURNS, side).start()

            pack(CORES * block(dist) + c, h)

        g = e - LAND_LAG

        @pl.when((g >= 0) & (g < packed))
        def _():
            expand(*turn(g))

        made = g - TURNS + 1

        @pl.when(made >= 0)
        def _():
            contract(*turn(made))
            send_back(*turn(made))

        homeward(made - HELD_LAG)

    for h in range(TURNS):
        lent_rest(h).wait_recv()

    @pl.loop(0, CUTS)
    def _(k):
        c = lax.div(k, TURNS)
        h = lax.rem(k, TURNS)
        mine = CORES * z + c
        total[:, span(h)] = mixed(mine, h)

        @pl.when(z > 0)
        def _():
            climb(mine, h).wait_recv()
            total[:, span(h)] += from_low[mine, :, span(h)].astype(jnp.float32)

        @pl.when(z < near)
        def _():
            sink(mine, h).wait_recv()
            total[:, span(h)] += from_high[mine, :, span(h)].astype(jnp.float32)

        @pl.when(c == core)
        def _():
            at = wide(core, h)
            out_ref[:, at] = (resid[:, at].astype(jnp.float32) + total[:, span(h)]).astype(
                jnp.bfloat16
            )

        @pl.when(c != core)
        def _():
            leaving[:, span(h)] = (
                lent_mid[:, span(h)].astype(jnp.float32) + total[:, span(h)]
            ).astype(jnp.bfloat16)
            settled(h).start()

    for h in range(TURNS):
        settled(h).wait_recv()
        out_ref[:, wide(1 - core, h)] = arrived[:, span(h)]

    @pl.loop(0, CORES * planes)
    def _(v):
        zs = lax.div(v, CORES)
        sent = toks.at[v]

        @pl.when((zs <= z) & (z < near))
        def _():
            tally(sent, zsend.at[0, v], zrecv.at[v, 0]).wait_send()

        @pl.when((zs >= z) & (z > 0))
        def _():
            tally(sent, zsend.at[1, v], zrecv.at[v, 0]).wait_send()

        @pl.when(zs != z)
        def _():
            tally(sent, csend.at[v], zrecv.at[v, 0]).wait_send()

        tally(stage.at[v, fan, :], psend.at[v], precv.at[v, 0]).wait_send()
        tally(stage.at[v, fan, :], rsend.at[v], rrecv.at[v, 0]).wait_send()

        @pl.when(lax.rem(v, CORES) == 0)
        def _():
            @pl.when((zs <= z) & (z < near))
            def _():
                tab_hop(zs, 0).wait_send()

            @pl.when((zs >= z) & (z > 0))
            def _():
                tab_hop(zs, 1).wait_send()

    tab_swap().wait_send()
    for h in range(TURNS):
        lent(h).wait_send()
        lent_rest(h).wait_send()
        settled(h).wait_send()

    for k in range(halves):
        swap(k, 0).wait_send()

    for side in range(2):

        @pl.when((sp < ends) if side else (sp > 0))
        def _():
            halo(side).wait_send()


def whole_layer(queries, kv, docs, sinks, gain, routes, shares, out_weight, hidden_in, weights, cap):
    planes = PLANES
    rows, width = hidden_in.shape
    tps = lax.axis_size("tp")
    stride = lax.axis_size("sp") // planes
    peers = stride * tps
    slots = peers * cap
    tok_here, heads_wide = queries.shape
    bf16, f32 = jnp.bfloat16, jnp.float32
    dma = pltpu.SemaphoreType.DMA
    vmem = pl.BlockSpec(memory_space=pltpu.VMEM)
    anywhere = pl.BlockSpec(memory_space=pl.ANY)
    hidden = weights[0].shape[1]
    units = CORES * planes
    half = width // CORES
    by_slot = pltpu.VMEM((units, slots, half), bf16)
    by_chip = pltpu.VMEM((units, slots // CORES, width), bf16)
    by_row = pltpu.VMEM((units, rows, half), bf16)
    chunks = dma((units, TURNS))
    each = dma((units,))
    halves = rows // WIN
    return pl.pallas_call(
        functools.partial(layer_kernel, planes, stride, tps, cap),
        out_shape=pltpu.VMEM((rows, width), bf16),
        in_specs=[vmem, vmem, vmem, pl.BlockSpec(memory_space=pltpu.SMEM), vmem, vmem, vmem]
        + [anywhere] * 5,
        out_specs=vmem,
        scratch_shapes=[
            pltpu.VMEM((tok_here + 2 * WIN, kv.shape[1] + LANES), bf16),
            pltpu.VMEM((halves + 1, WIN, heads_wide), bf16),
            pltpu.VMEM((rows, out_weight.shape[0]), bf16),
            pltpu.VMEM((rows, width), bf16),
            pltpu.VMEM((WIN, 3 * WIN), f32),
            pltpu.VMEM((rows, LANES), f32),
            pltpu.VMEM((rows, half), bf16),
            pltpu.VMEM((rows, half), bf16),
            pltpu.VMEM((rows, half), bf16),
            pltpu.VMEM((rows, half), bf16),
            by_row, by_slot, by_chip, by_chip, by_slot, by_row, by_row, by_row,
            pltpu.VMEM((width, hidden), bf16),
            pltpu.VMEM((width, hidden), bf16),
            pltpu.VMEM((hidden, width), bf16),
            pltpu.VMEM((slots // CORES, hidden), f32),
            pltpu.VMEM((slots // CORES, hidden), f32),
            pltpu.VMEM((slots // CORES, hidden), bf16),
            pltpu.VMEM((units, rows, slots), bf16),
            pltpu.VMEM((rows, width), f32),
            pltpu.VMEM((units, 8, rows), f32),
            dma((2, units)), chunks, each, chunks, each, chunks, each, chunks, chunks,
            dma((2, planes)), dma((planes,)), dma((3,)),
            dma((2,)), dma((2,)), dma((halves,)), dma((halves,)), dma((units + 1,)),
            dma((3, TURNS)), dma((3, TURNS)), dma, dma,
        ],
        compiler_params=pltpu.CompilerParams(
            collective_id=0, has_side_effects=True, vmem_limit_bytes=57 * 1024 * 1024
        ),
        name="layer",
    )(queries, kv, docs, sinks, gain, routes, shares, out_weight, hidden_in, *weights)


def expert_rows(arrived, gate_w, up_w, down_w):
    width = arrived.shape[-1]
    flat_rows = arrived.reshape(-1, width)
    gate = jnp.dot(flat_rows, gate_w, preferred_element_type=jnp.float32)
    upper = jnp.dot(flat_rows, up_w, preferred_element_type=jnp.float32)
    expert_hidden = (jax.nn.silu(gate) * upper).astype(jnp.bfloat16)
    result = jnp.dot(expert_hidden, down_w, preferred_element_type=jnp.float32).astype(jnp.bfloat16)
    return result.reshape(arrived.shape[:-1] + (result.shape[-1],))


def shards(
    queries,
    keys_values,
    doc_ids,
    head_sink,
    out_weight,
    hidden_in,
    norm_gain,
    expert_gate,
    expert_up,
    expert_down,
    routes,
    route_weight,
):
    tok_here = queries.shape[0]
    heads_here = head_sink.shape[0]
    kv_here = keys_values.shape[1]
    group = heads_here // kv_here
    head_dim = keys_values.shape[2] // 2
    topk = routes.shape[1]
    local_rows, width = hidden_in.shape
    sp_count = lax.axis_size("sp")
    tp_count = lax.axis_size("tp")
    expert_count = sp_count * tp_count
    capacity = 2 * local_rows * topk // expert_count
    if (
        capacity % 16 == 0
        and sp_count % PLANES == 0
        and topk == 2
        and tp_count == 2
        and 2 * head_dim == LANES
        and group % 2 == 0
        and local_rows % WIN == 0
        and local_rows > WIN
        and out_weight.shape[0] == PLANES * local_rows
        and queries.shape[1] % local_rows == 0
        and sp_count // PLANES % CORES == 0
    ):
        return whole_layer(
            queries,
            keys_values.reshape(tok_here, -1),
            doc_ids.reshape(1, tok_here),
            head_sink,
            norm_gain.reshape(1, width),
            routes.T,
            route_weight.T,
            out_weight,
            hidden_in,
            (expert_gate[0], expert_up[0], expert_down[0]),
            capacity,
        )
    docs_wide = jnp.broadcast_to(
        doc_ids.astype(jnp.bfloat16)[:, None], (tok_here, keys_values.shape[2])
    )
    slab = jnp.concatenate([keys_values.reshape(tok_here, -1), docs_wide], axis=1)
    slab = with_halo(slab, "sp", WIN)
    kv_ext = slab[:, : kv_here * keys_values.shape[2]].reshape(
        -1, kv_here, keys_values.shape[2]
    )
    docs_ext = slab[:, kv_here * keys_values.shape[2]].astype(jnp.int32)
    offset = lax.axis_index("sp") * tok_here
    seq_total = lax.axis_size("sp") * tok_here
    span_rows = min(512, tok_here)
    sink_logit = head_sink.reshape(kv_here, group)[:, :, None, None]

    def one_span(span_index):
        first_row = span_index * span_rows
        q_span = queries.reshape(span_rows, kv_here, group, head_dim)
        scores = jnp.einsum(
            "qhgd,khd->hgqk", q_span, kv_ext[..., :head_dim], preferred_element_type=jnp.float32
        ) * HD ** (-0.5)
        query_pos = offset + first_row + jnp.arange(span_rows, dtype=jnp.int32)
        key_pos = offset + first_row - WIN + jnp.arange(span_rows + 2 * WIN, dtype=jnp.int32)
        inside = (key_pos >= 0) & (key_pos < seq_total)
        allowed = (
            (jnp.abs(key_pos[None, :] - query_pos[:, None]) <= WIN)
            & inside[None, :]
            & (docs_ext[None, :] == doc_ids[:, None])
        )
        masked = jnp.where(allowed, scores, -1e30)
        row_max = jnp.maximum(masked.max(-1, keepdims=True), sink_logit)
        exp_scores = jnp.where(allowed, jnp.exp(masked - row_max), 0.0)
        total_mass = exp_scores.sum(-1, keepdims=True) + jnp.exp(sink_logit - row_max)
        weights = (exp_scores / total_mass).astype(jnp.bfloat16)
        outcome = jnp.einsum(
            "hgqk,khd->qhgd", weights, kv_ext[..., head_dim:], preferred_element_type=jnp.float32
        )
        return outcome.astype(jnp.bfloat16).reshape(span_rows, heads_here * head_dim)

    attended = lax.map(one_span, jnp.arange(tok_here // span_rows, dtype=jnp.int32)).reshape(
        tok_here, -1
    )
    if lax.axis_size("tp") == 2:
        tp = lax.axis_index("tp")
        half = tok_here // 2
        mine = lax.dynamic_slice_in_dim(attended, tp * half, half, 0)
        other = lax.ppermute(
            lax.dynamic_slice_in_dim(attended, (1 - tp) * half, half, 0), "tp", [(0, 1), (1, 0)]
        )
        gathered = jnp.concatenate(
            [jnp.where(tp == 0, mine, other), jnp.where(tp == 0, other, mine)], axis=1
        )
    else:
        gathered = lax.all_to_all(attended, "tp", split_axis=0, concat_axis=1, tiled=True)
    projected = jnp.dot(gathered, out_weight, preferred_element_type=jnp.float32)
    mid_wide = (hidden_in.astype(jnp.float32) + projected).astype(jnp.bfloat16).astype(jnp.float32)
    normed = (
        mid_wide
        * lax.rsqrt(jnp.mean(mid_wide * mid_wide, axis=-1, keepdims=True) + 1e-06)
        * norm_gain
    ).astype(jnp.bfloat16)
    flat_routes = routes.reshape(-1)
    one_hot = (flat_routes[:, None] == jnp.arange(expert_count, dtype=jnp.int32)[None, :]).astype(
        jnp.int32
    )
    slot_rank = (jnp.cumsum(one_hot, axis=0) * one_hot).sum(-1) - 1
    slot_index = flat_routes * capacity + slot_rank
    repeated = jnp.repeat(normed, topk, axis=0)
    buffer_rows = (
        jnp.zeros((expert_count * capacity, width), jnp.bfloat16).at[slot_index].set(repeated)
    )
    sent = buffer_rows.reshape(expert_count, capacity, width)
    finished = expert_rows(
        lax.all_to_all(sent, ("sp", "tp"), split_axis=0, concat_axis=0, tiled=True),
        expert_gate[0],
        expert_up[0],
        expert_down[0],
    )
    returned = lax.all_to_all(finished, ("sp", "tp"), split_axis=0, concat_axis=0, tiled=True)
    returned = returned.reshape(expert_count * capacity, width)
    picked = returned[slot_index].astype(jnp.float32).reshape(local_rows, topk, width)
    mixture = jnp.sum(picked * route_weight[..., None], axis=1)
    return (mid_wide + mixture).astype(jnp.bfloat16)


def solution(mesh):
    placed = (
        P("sp", "tp"),
        P("sp", "tp", None),
        P("sp"),
        P("tp"),
        P(),
        P(("sp", "tp"), None),
        P(),
        P(("sp", "tp"), None, None),
        P(("sp", "tp"), None, None),
        P(("sp", "tp"), None, None),
        P(("sp", "tp"), None),
        P(("sp", "tp"), None),
    )
    return jax.shard_map(
        shards, mesh=mesh, in_specs=placed, out_specs=P(("sp", "tp"), None), check_vma=False
    )
```
